512 devices in a mesh: ep: 32 (over z, x), tp: 16 (over y, core).
Axes of the slice: x: 4, y: 8, z: 8, core: 2. Of those that a mesh axis runs over, the one named last changes fastest.
Arguments:
- queries: bfloat16 [4096, 1536], P('ep', 'tp'), may hold values from -400 to 400
- token_latents: bfloat16 [4096, 512], P('ep'), may hold values from -6 to 6
- key_rotary: bfloat16 [4096, 32], P('ep'), may hold values from -6 to 6
- latent_norm_gain: float32 [512], replicated, may hold values from 0.1 to 1.9
- latent_up_weight: bfloat16 [512, 2048], P(None, 'tp'), may hold values from -0.25 to 0.25
- w_out: bfloat16 [1024, 2048], P('tp'), may hold values from -0.1875 to 0.1875
- tokens_b: bfloat16 [4096, 2048], P('ep'), may hold values from -6 to 6
- moe_gain: float32 [2048], replicated, may hold values from 0.1 to 1.9
- group_logits: float32 [4096, 4], P('ep'), may hold values from -6 to 6
- inner_logits: float32 [4096, 2], P('ep'), may hold values from -6 to 6
- expert_pick: int32 [4096, 2], P('ep'), may hold values from 0 to 31, as said below
- w_gate: bfloat16 [32, 2048, 4096], P('ep', None, 'tp'), may hold values from -0.125 to 0.125
- w_up: bfloat16 [32, 2048, 4096], P('ep', None, 'tp'), may hold values from -0.125 to 0.125
- w_down: bfloat16 [32, 4096, 2048], P('ep', 'tp'), may hold values from -0.09375 to 0.09375
Outputs:
- mixer_out: bfloat16 [4096, 2048], P(('ep', 'tp'))
- expert_out: bfloat16 [4096, 2048], P('ep', 'tp')
The draws below stay inside these ranges and needn't reach their ends.
Inputs may be any that keep to these rules, and one draw needn't show every extreme that they name: `expert_pick`: each row names two different experts of one group, a group being 8 consecutive experts. Among the 128 rows of one index of ep no expert is named more than 16 times; in every draw some expert is named exactly 16 times by the rows of every index of ep.
All inputs are finite; a program needn't handle non-finite values.
Results may differ from the reference program's by a relative error of at most 0.018.
The reference program's roundings to bfloat16 on the way count: a program that leaves them out, or rounds other values in their place, can miss the bound.
Values may be sent and summed in bfloat16 or wider, within the bound.
No kernel may reach another device: no remote copies, remote signals or barrier semaphores. Data moves between devices by JAX's collectives and lax.ppermute only.
A program may use at most 64 MiB of HBM per device.

```python
import jax
import jax.numpy as jnp
from jax import lax

D = 2048
HEAD_TOTAL = 16
PLAIN_HEAD_SIZE = 64
D_ROPE = 32
VALUE_HEAD_SIZE = 64
LATENT_WIDTH = 512
FF = 4096
GROUPS = 4
TOP = 2
SEGMENT = 64
TOK_B = 128
ATTENTION_TOKENS = 4096
TOKENS_B = 4096
EXPERTS = 32
EPG = 8
CAP = 16
HEADS_DEV = 1
WIDTH_DEV = 256
N_TP = 16


def draw_queries(key, part):
    drawn = jax.random.normal(key, (ATTENTION_TOKENS, HEAD_TOTAL * (PLAIN_HEAD_SIZE + D_ROPE)), jnp.float32)
    return jnp.clip(drawn, -400.0, 400.0).astype(jnp.bfloat16)


def draw_expert_pick(key, part):
    per_group = EXPERTS // GROUPS
    block_count = TOKENS_B // TOK_B
    heavy_group = jax.random.randint(jax.random.fold_in(key, 1), (), 0, GROUPS)
    block_keys = jax.random.split(jax.random.fold_in(key, 2), block_count)

    def one_block(block_key):
        cut_key, perm_key, row_key = jax.random.split(block_key, 3)
        half_rows = TOK_B // 2
        cut_points = jnp.sort(jax.random.randint(cut_key, (GROUPS - 2,), 0, half_rows + 1))
        edge_list = jnp.concatenate([jnp.zeros((1,), jnp.int32), cut_points.astype(jnp.int32), jnp.full((1,), half_rows, jnp.int32)])
        others = edge_list[1:] - edge_list[:-1]
        group_rank = (jnp.arange(GROUPS, dtype=jnp.int32) - heavy_group - 1) % GROUPS
        group_loads = jnp.where(group_rank == GROUPS - 1, half_rows, others[jnp.minimum(group_rank, GROUPS - 2)])
        group_ends = jnp.cumsum(group_loads)
        position = jnp.arange(TOK_B, dtype=jnp.int32)
        group_index = jnp.sum((position[:, None] >= group_ends[None, :]).astype(jnp.int32), axis=1)
        inside = position - (group_ends - group_loads)[group_index]
        perm_scores = jax.random.randint(perm_key, (GROUPS, per_group), 0, 1 << 20) * per_group
        perm_scores = perm_scores + jnp.arange(per_group, dtype=jnp.int32)[None, :]
        perm_table = jnp.argsort(perm_scores, axis=1).astype(jnp.int32)
        first_pick = perm_table[group_index, inside % per_group]
        second_pick = perm_table[group_index, (inside + 1) % per_group]
        both_picks = jnp.stack([group_index * per_group + first_pick, group_index * per_group + second_pick], axis=1)
        return jax.random.permutation(row_key, both_picks, axis=0)
    return jax.vmap(one_block)(block_keys).reshape(TOKENS_B, 2).astype(jnp.int32)


def block_levels(stream_key, dims, cuts, smallest, high):
    def one(dim, parts):
        draws = jax.random.uniform(jax.random.fold_in(jax.random.fold_in(stream_key, 6), dim), (parts,), jnp.float32, smallest / len(cuts), high / len(cuts))
        return jnp.repeat(jnp.exp(draws), dims[dim] // parts).reshape((-1,) + (1,) * (len(dims) - dim - 1))

    level = one(*cuts[0])
    for cut in cuts[1:]:
        level = level * one(*cut)
    return level


def centred(key, extent, deviation, reach, shards=(), kind=jnp.bfloat16):
    entries = deviation * jax.random.normal(key, extent, jnp.float32)
    if shards:
        entries = entries * block_levels(key, extent, shards, -0.22, 0.18)
    return jnp.clip(entries, -reach, reach).astype(kind)


def setup_inputs(seed: int = 0) -> dict:
    splits = jax.random.split(jax.random.key(seed), 15)
    queries = draw_queries(jax.random.fold_in(splits[14], 71), 0)
    token_latents = centred(splits[1], (ATTENTION_TOKENS, LATENT_WIDTH), 1.0, 6.0, ((0, 32),))
    key_rotary = centred(splits[2], (ATTENTION_TOKENS, D_ROPE), 1.0, 6.0, ((0, 32),))
    latent_norm_gain = jnp.clip(1.0 + 0.18 * jax.random.normal(splits[3], (LATENT_WIDTH,), jnp.float32), 0.1, 1.9)
    latent_up_weight = centred(splits[4], (LATENT_WIDTH, HEAD_TOTAL * (PLAIN_HEAD_SIZE + VALUE_HEAD_SIZE)), LATENT_WIDTH ** -0.5, 0.25, ((1, 16),))
    w_out = centred(splits[5], (HEAD_TOTAL * VALUE_HEAD_SIZE, D), (HEAD_TOTAL * VALUE_HEAD_SIZE) ** -0.5, 0.1875, ((0, 16),))
    tokens_b = centred(splits[6], (TOKENS_B, D), 1.0, 6.0, ((0, 32),))
    moe_gain = jnp.clip(1.0 + 0.18 * jax.random.normal(splits[7], (D,), jnp.float32), 0.1, 1.9)
    group_logits = centred(splits[8], (TOKENS_B, GROUPS), 1.5, 6.0, ((0, 32),), jnp.float32)
    inner_logits = centred(splits[9], (TOKENS_B, TOP), 1.5, 6.0, ((0, 32),), jnp.float32)
    expert_pick = draw_expert_pick(jax.random.fold_in(splits[14], 71), 0)
    w_gate = centred(splits[11], (EXPERTS, D, FF), D ** -0.5, 0.125, ((0, 32), (2, 16)))
    w_up = centred(splits[12], (EXPERTS, D, FF), D ** -0.5, 0.125, ((0, 32), (2, 16)))
    w_down = centred(splits[13], (EXPERTS, FF, D), FF ** -0.5, 0.09375, ((0, 32), (1, 16)))
    return dict(queries=queries, token_latents=token_latents, key_rotary=key_rotary, latent_norm_gain=latent_norm_gain, latent_up_weight=latent_up_weight, w_out=w_out, tokens_b=tokens_b, moe_gain=moe_gain, group_logits=group_logits, inner_logits=inner_logits, expert_pick=expert_pick, w_gate=w_gate, w_up=w_up, w_down=w_down)


def rotate(values, positions):
    half_size = values.shape[-1] // 2
    frequency = jnp.power(10000.0, -jnp.arange(half_size, dtype=jnp.float32) * 2.0 / values.shape[-1])
    angles = positions[:, None] * frequency[None, :]
    if values.ndim == 3:
        angles = angles[:, None, :]
    cosine = jnp.cos(angles)
    sine_part = jnp.sin(angles)
    first_half = values[..., :half_size]
    second_half = values[..., half_size:]
    return jnp.concatenate([first_half * cosine - second_half * sine_part, second_half * cosine + first_half * sine_part], axis=-1)

def mixer(queries, token_latents, key_rotary, latent_norm_gain, latent_up_weight, w_out):
    length = queries.shape[0]
    positions = jnp.arange(length, dtype=jnp.float32)
    query_heads = queries.reshape(length, HEAD_TOTAL, PLAIN_HEAD_SIZE + D_ROPE)
    q_plain = query_heads[:, :, :PLAIN_HEAD_SIZE]
    q_turned = rotate(query_heads[:, :, PLAIN_HEAD_SIZE:].astype(jnp.float32), positions).astype(jnp.bfloat16)
    latent = token_latents.astype(jnp.float32)
    normed_latent = (latent * lax.rsqrt(lax.optimization_barrier(jnp.mean(latent * latent, axis=-1, keepdims=True)) + 1e-06) * latent_norm_gain).astype(jnp.bfloat16)
    key_value = jnp.dot(normed_latent, latent_up_weight, preferred_element_type=jnp.float32).astype(jnp.bfloat16)
    key_value = key_value.reshape(length, HEAD_TOTAL, PLAIN_HEAD_SIZE + VALUE_HEAD_SIZE)
    k_turned = rotate(key_rotary.astype(jnp.float32), positions).astype(jnp.bfloat16)
    block_rows = 512 if length % 512 == 0 else length
    blocks = length // block_rows
    segment_all = jnp.arange(length, dtype=jnp.int32) // SEGMENT
    scale_factor = (PLAIN_HEAD_SIZE + D_ROPE) ** (-0.5)

    def one_head(head_args):
        plain_h, turned_h, key_h, value_h = head_args

        def one_block(block_args):
            plain_b, turned_b, first_row = block_args
            scores = jnp.dot(plain_b, key_h.T, preferred_element_type=jnp.float32)
            scores = scores + jnp.dot(turned_b, k_turned.T, preferred_element_type=jnp.float32)
            scores = scores * scale_factor
            query_segment = (first_row + jnp.arange(block_rows, dtype=jnp.int32)) // SEGMENT
            allowed = query_segment[:, None] >= segment_all[None, :]
            scores = jnp.where(allowed, scores, -jnp.inf)
            row_max = lax.optimization_barrier(jnp.max(scores, axis=-1, keepdims=True))
            exp_scores = jnp.exp(scores - row_max)
            denominator = lax.optimization_barrier(jnp.sum(exp_scores, axis=-1, keepdims=True))
            numerator = jnp.dot(exp_scores.astype(jnp.bfloat16), value_h, preferred_element_type=jnp.float32)
            return (numerator / denominator).astype(jnp.bfloat16)
        starts = jnp.arange(blocks, dtype=jnp.int32) * block_rows
        result = lax.map(one_block, (plain_h.reshape(blocks, block_rows, PLAIN_HEAD_SIZE), turned_h.reshape(blocks, block_rows, D_ROPE), starts))
        return result.reshape(length, VALUE_HEAD_SIZE)
    heads_out = lax.map(one_head, (q_plain.transpose(1, 0, 2), q_turned.transpose(1, 0, 2), key_value[:, :, :PLAIN_HEAD_SIZE].transpose(1, 0, 2), key_value[:, :, PLAIN_HEAD_SIZE:].transpose(1, 0, 2)))
    attended = heads_out.transpose(1, 0, 2).reshape(length, HEAD_TOTAL * VALUE_HEAD_SIZE)
    group_cols = HEADS_DEV * VALUE_HEAD_SIZE

    def add_group(group_index, running):
        first_col = (group_index * group_cols).astype(jnp.int32)
        columns = lax.dynamic_slice_in_dim(attended, first_col, group_cols, 1)
        weight_rows = lax.dynamic_slice_in_dim(w_out, first_col, group_cols, 0)
        partial_value = jnp.dot(columns, weight_rows, preferred_element_type=jnp.float32).astype(jnp.bfloat16)
        partial_value = lax.optimization_barrier(partial_value)
        return running + partial_value.astype(jnp.float32)
    total = lax.fori_loop(0, N_TP, add_group, jnp.zeros((length, D), jnp.float32))
    return total.astype(jnp.bfloat16)

def experts_half(tokens_b, moe_gain, group_logits, inner_logits, expert_pick, w_gate, w_up, w_down):
    total_rows = tokens_b.shape[0]
    values_f = tokens_b.astype(jnp.float32)
    centered = values_f - lax.optimization_barrier(jnp.mean(values_f, axis=-1, keepdims=True))
    variance = lax.optimization_barrier(jnp.mean(centered * centered, axis=-1, keepdims=True))
    normed = (centered * lax.rsqrt(variance + 1e-05) * moe_gain).astype(jnp.bfloat16)
    home_group = expert_pick[:, 0] // EPG
    own_logit = lax.optimization_barrier(jnp.sum(jnp.where(jnp.arange(GROUPS, dtype=jnp.int32)[None, :] == home_group[:, None], group_logits, 0.0), axis=1))
    group_share = 1.0 / lax.optimization_barrier(jnp.sum(jnp.exp(group_logits - own_logit[:, None]), axis=1))
    logit_gap = inner_logits[:, 0] - inner_logits[:, 1]
    route_weight = group_share[:, None] * jnp.stack([jax.nn.sigmoid(logit_gap), jax.nn.sigmoid(-logit_gap)], axis=1)
    slots_all = EXPERTS * CAP

    def one_expert(expert_id, running):
        matches = expert_pick == expert_id.astype(jnp.int32)
        named = jnp.any(matches, axis=1)
        picked_rows = jnp.nonzero(named, size=slots_all, fill_value=0)[0].astype(jnp.int32)
        live = jnp.arange(slots_all, dtype=jnp.int32) < jnp.sum(named.astype(jnp.int32))
        inputs = normed[picked_rows]
        gate_proj = jnp.dot(inputs, w_gate[expert_id], preferred_element_type=jnp.float32)
        up_proj = jnp.dot(inputs, w_up[expert_id], preferred_element_type=jnp.float32)
        hidden = (jax.nn.silu(gate_proj) * up_proj).astype(jnp.bfloat16)
        pieces = hidden.reshape(slots_all, N_TP, WIDTH_DEV).astype(jnp.float32)
        down_parts = w_down[expert_id].reshape(N_TP, WIDTH_DEV, D).astype(jnp.float32)
        partial_value = jnp.einsum('ntf,tfd->ntd', pieces, down_parts).astype(jnp.bfloat16)
        partial_value = lax.optimization_barrier(partial_value)
        result = lax.optimization_barrier(jnp.sum(partial_value.astype(jnp.float32), axis=1)).astype(jnp.bfloat16)
        result = lax.optimization_barrier(result)
        weight = lax.optimization_barrier(jnp.sum(jnp.where(matches[picked_rows], route_weight[picked_rows], 0.0), axis=1))
        weight = jnp.where(live, weight, 0.0)
        return running.at[picked_rows].add(weight[:, None] * result.astype(jnp.float32))
    total = lax.fori_loop(0, EXPERTS, one_expert, jnp.zeros((total_rows, D), jnp.float32))
    return total.astype(jnp.bfloat16)

def reference(queries, token_latents, key_rotary, latent_norm_gain, latent_up_weight, w_out, tokens_b, moe_gain, group_logits, inner_logits, expert_pick, w_gate, w_up, w_down):
    mixer_out = mixer(queries, token_latents, key_rotary, latent_norm_gain, latent_up_weight, w_out)
    expert_out = experts_half(tokens_b, moe_gain, group_logits, inner_logits, expert_pick, w_gate, w_up, w_down)
    return (mixer_out, expert_out)
```

```python
import functools

import jax
import jax.numpy as jnp
from jax import lax
from jax.experimental import pallas as pl
from jax.experimental.pallas import tpu as pltpu
from jax.sharding import Mesh, PartitionSpec as P

PLAIN = 64
ROT = 32
VAL = 64
SEG = 64
GROUPS = 4
BF = jnp.bfloat16
F32 = jnp.float32
VMEM_LIMIT = 48 * 1024 * 1024


def split3(v):
    hi = v.astype(BF).astype(F32)
    rest = v - hi
    mid = rest.astype(BF).astype(F32)
    return hi, mid, rest - mid


def attend_kernel(where_ref, q0, q1, q2, q3, kv_ref, o0, o1, o2, o3):
    z = where_ref[0]
    x = where_ref[1]
    zs, _, tok = kv_ref.shape
    xs = 4
    keys = jnp.concatenate([kv_ref[b, : PLAIN + ROT, :] for b in range(zs)], axis=1)
    vals = jnp.concatenate([kv_ref[b, PLAIN + ROT :, :] for b in range(zs)], axis=1)
    col = lax.broadcasted_iota(jnp.int32, (1, zs * tok), 1)
    key_seg = ((col // tok) * xs + x) * (tok // SEG) + (col % tok) // SEG
    row = lax.broadcasted_iota(jnp.int32, (tok, 1), 0)
    scale = (PLAIN + ROT) ** -0.5
    lane = lax.broadcasted_iota(jnp.int32, (tok, 128), 1)
    for k, (q_ref, o_ref) in enumerate(((q0, o0), (q1, o1), (q2, o2), (q3, o3))):
        xq = lax.rem(x + xs - k, xs)
        q_seg = (z * xs + xq) * (tok // SEG) + row // SEG
        s = jnp.dot(q_ref[...], keys, preferred_element_type=F32) * scale
        s = jnp.where(q_seg >= key_seg, s, -3e38)
        m = jnp.maximum(jnp.max(s, axis=1, keepdims=True), -1e30)
        p = jnp.exp(s - m)
        l = jnp.sum(p, axis=1, keepdims=True)
        acc = lax.dot_general(p.astype(BF), vals, (((1,), (1,)), ((), ())), preferred_element_type=F32)
        out = jnp.concatenate([acc, jnp.zeros((tok, 128 - VAL), F32)], axis=1)
        for i, piece in enumerate(split3(m) + split3(l)):
            out = jnp.where(lane == VAL + i, piece, out)
        o_ref[...] = out.astype(BF)


def mix_kernel(c_ref, a0, a1, a2, a3, w_ref, keep_ref, send_ref, res_ref):
    c = c_ref[0]
    parts = [r[...].astype(F32) for r in (a0, a1, a2, a3)]
    ms = [p[:, VAL : VAL + 1] + p[:, VAL + 1 : VAL + 2] + p[:, VAL + 2 : VAL + 3] for p in parts]
    ls = [p[:, VAL + 3 : VAL + 4] + p[:, VAL + 4 : VAL + 5] + p[:, VAL + 5 : VAL + 6] for p in parts]
    m = functools.reduce(jnp.maximum, ms)
    total = 0.0
    denom = 0.0
    for p, mp, lp in zip(parts, ms, ls):
        w = jnp.exp(mp - m)
        total = total + w * p[:, :VAL]
        denom = denom + w * lp
    attended = (total / denom).astype(BF)
    res_ref[...] = jnp.dot(attended, w_ref[...], preferred_element_type=F32)
    for y in range(keep_ref.shape[0]):
        keep_ref[y] = res_ref[pl.ds(pl.multiple_of(16 * y + 8 * c, 8), 8), :].astype(BF)
        send_ref[y] = res_ref[pl.ds(pl.multiple_of(16 * y + 8 * (1 - c), 8), 8), :].astype(BF)


def vm(n):
    return [pl.BlockSpec(memory_space=pltpu.VMEM)] * n


def per_device(
    queries, token_latents, key_rotary, latent_norm_gain, latent_up_weight, w_out,
    tokens_b, moe_gain, group_logits, inner_logits, expert_pick, w_gate, w_up, w_down,
):
    ep = ("z", "x")
    zs, xs, ys = lax.axis_size("z"), lax.axis_size("x"), lax.axis_size("y")
    z, x, c = lax.axis_index("z"), lax.axis_index("x"), lax.axis_index("c")
    tok = queries.shape[0]
    width = tokens_b.shape[1]
    experts = zs * xs
    half = 8
    swap = [(0, 1), (1, 0)]

    positions = ((z * xs + x) * tok + jnp.arange(tok, dtype=jnp.int32)).astype(F32)
    freq = jnp.power(10000.0, -jnp.arange(ROT // 2, dtype=F32) * 2.0 / ROT)
    ang = positions[:, None] * freq[None, :]
    cos, sin = jnp.cos(ang), jnp.sin(ang)

    def rope(v):
        v = v.astype(F32)
        a, b = v[:, : ROT // 2], v[:, ROT // 2 :]
        return jnp.concatenate([a * cos - b * sin, b * cos + a * sin], axis=1).astype(BF)

    lat = token_latents.astype(F32)
    lat = (lat * lax.rsqrt(jnp.mean(lat * lat, axis=-1, keepdims=True) + 1e-06) * latent_norm_gain).astype(BF)
    kv_t = lax.dot_general(
        latent_up_weight, lat, (((0,), (1,)), ((), ())), preferred_element_type=F32
    ).astype(BF)
    k_turned = rope(key_rotary)
    pack = jnp.concatenate([kv_t[:PLAIN], k_turned.T, kv_t[PLAIN:]], axis=0)
    kv_all = lax.all_to_all(
        jnp.broadcast_to(pack[None], (zs,) + pack.shape), "z", 0, 0, tiled=True
    )

    q_own = jnp.concatenate([queries[:, :PLAIN], rope(queries[:, PLAIN:])], axis=1)
    qs = [q_own] + [
        lax.ppermute(q_own, "x", [(i, (i + k) % xs) for i in range(xs)]) for k in range(1, xs)
    ]

    vals = tokens_b.astype(F32)
    cen = vals - jnp.mean(vals, axis=-1, keepdims=True)
    var = jnp.mean(cen * cen, axis=-1, keepdims=True)
    normed = (cen * lax.rsqrt(var + 1e-05) * moe_gain).astype(BF)
    pick_t = expert_pick.T
    eid = jnp.arange(experts, dtype=jnp.int32)[:, None]
    hit0 = pick_t[0:1] == eid
    hit1 = pick_t[1:2] == eid
    hit = hit0 | hit1
    rr = jnp.arange(tok, dtype=jnp.int32)
    upper = (rr[:, None] < rr[None, :]).astype(BF)
    rank = jnp.dot(hit.astype(BF), upper, preferred_element_type=F32)
    code = jnp.where(hit, rank.astype(jnp.int32), -1)
    slot = half * c + jnp.arange(half, dtype=jnp.int32)
    sel = code[:, None, :] == slot[None, :, None]
    onehot = sel.astype(BF).reshape(experts * half, tok)
    outbound = jnp.dot(onehot, normed, preferred_element_type=F32).astype(BF)
    arrived = lax.all_to_all(
        outbound.reshape(experts, half, width), ep, 0, 0, tiled=True
    ).reshape(experts * half, width)

    wg, wu, wd = w_gate[0], w_up[0], w_down[0]
    wg2, wu2, wd2 = (lax.ppermute(w, "c", swap) for w in (wg, wu, wd))

    where = jnp.stack([z, x]).astype(jnp.int32)
    parts = pl.pallas_call(
        attend_kernel,
        out_shape=[jax.ShapeDtypeStruct((tok, 128), BF)] * xs,
        in_specs=[pl.BlockSpec(memory_space=pltpu.SMEM)] + vm(5),
        out_specs=vm(4),
        name="attend",
        compiler_params=pltpu.CompilerParams(vmem_limit_bytes=VMEM_LIMIT),
    )(where, *qs, kv_all)
    back = [parts[0]] + [
        lax.ppermute(parts[k], "x", [(i, (i - k) % xs) for i in range(xs)]) for k in range(1, xs)
    ]
    keep_mix, send_mix = pl.pallas_call(
        mix_kernel,
        out_shape=[jax.ShapeDtypeStruct((ys, 8, width), BF)] * 2,
        in_specs=[pl.BlockSpec(memory_space=pltpu.SMEM)] + vm(5),
        out_specs=vm(2),
        scratch_shapes=[pltpu.VMEM((tok, width), F32)],
        name="mix",
        compiler_params=pltpu.CompilerParams(vmem_limit_bytes=VMEM_LIMIT),
    )(c.reshape(1).astype(jnp.int32), *back, w_out)
    got_mix = lax.ppermute(send_mix, "c", swap)
    mix_half = (keep_mix.astype(F32) + got_mix.astype(F32)).astype(BF)

    def hidden(g_w, u_w):
        g = jnp.dot(arrived, g_w, preferred_element_type=F32)
        u = jnp.dot(arrived, u_w, preferred_element_type=F32)
        return (g / (1.0 + jnp.exp(-g)) * u).astype(BF)

    result = (
        jnp.dot(hidden(wg, wu), wd, preferred_element_type=F32)
        + jnp.dot(hidden(wg2, wu2), wd2, preferred_element_type=F32)
    ).astype(BF)
    returned = lax.all_to_all(
        result.reshape(experts, half, width), ep, 0, 0, tiled=True
    ).reshape(experts * half, width)

    gl = group_logits.T
    home = pick_t[0:1] // (experts // GROUPS)
    own = jnp.sum(jnp.where(jnp.arange(GROUPS, dtype=jnp.int32)[:, None] == home, gl, 0.0), axis=0, keepdims=True)
    share = 1.0 / jnp.sum(jnp.exp(gl - own), axis=0, keepdims=True)
    gap = (inner_logits[:, 0] - inner_logits[:, 1])[None, :]
    weight = jnp.where(hit0, share * jax.nn.sigmoid(gap), 0.0) + jnp.where(hit1, share * jax.nn.sigmoid(-gap), 0.0)
    w_hi = lax.reduce_precision(weight, 8, 7)
    w_lo = weight - w_hi

    def spread(w):
        return jnp.where(sel, w[:, None, :], 0.0).astype(BF).reshape(experts * half, tok)

    tn = (((0,), (0,)), ((), ()))
    combined = lax.dot_general(spread(w_hi), returned, tn, preferred_element_type=F32) + lax.dot_general(
        spread(w_lo), returned, tn, preferred_element_type=F32
    )
    combined = combined.reshape(tok, ys, 2, 128)
    keep = lax.dynamic_index_in_dim(combined, c, 2, keepdims=False).transpose(1, 0, 2)
    send = lax.dynamic_index_in_dim(combined, 1 - c, 2, keepdims=False).transpose(1, 0, 2).astype(BF)
    got = lax.ppermute(send, "c", swap)
    moe_half = (keep + got.astype(F32)).astype(BF)

    mix_rows = mix_half.reshape(ys, 8, width // 128, 128).transpose(0, 2, 1, 3).reshape(ys, width // 16, 128)
    last = lax.all_to_all(jnp.concatenate([moe_half, mix_rows], axis=1), "y", 0, 0, tiled=True)
    summed = jnp.sum(last.astype(F32), axis=0).astype(BF)
    expert_out = summed[:tok]
    mixer_out = summed[tok:].reshape(width // 128, 8, 128).transpose(1, 0, 2).reshape(8, width)
    return mixer_out, expert_out


def solution(mesh):
    fine = Mesh(mesh.devices.reshape(8, 4, 8, 2), ("z", "x", "y", "c"))
    e, t = ("z", "x"), ("y", "c")
    in_specs = (
        P(e, t), P(e, None), P(e, None), P(), P(None, t), P(t, None), P(e, None), P(),
        P(e, None), P(e, None), P(e, None), P(e, None, t), P(e, None, t), P(e, t, None),
    )
    out_specs = (P(e + t, None), P(e, t))
    return jax.shard_map(per_device, mesh=fine, in_specs=in_specs, out_specs=out_specs, check_vma=False)
```

```python
import functools

import jax
import jax.numpy as jnp
from jax import lax
from jax.experimental import pallas as pl
from jax.experimental.pallas import tpu as pltpu
from jax.sharding import Mesh, PartitionSpec as P

PLAIN = 64
ROT = 32
VAL = 64
SEG = 64
GROUPS = 4
BF = jnp.bfloat16
F32 = jnp.float32
MIB = 1024 * 1024


def split3(v):
    hi = v.astype(BF).astype(F32)
    rest = v - hi
    mid = rest.astype(BF).astype(F32)
    return hi, mid, rest - mid


def turn(v, cos, sin):
    a, b = v[: ROT // 2].astype(F32), v[ROT // 2 :].astype(F32)
    return jnp.concatenate([a * cos - b * sin, b * cos + a * sin], axis=0)


def fetch(pairs, sems):
    copies = [pltpu.make_async_copy(src, dst, sems.at[i]) for i, (src, dst) in enumerate(pairs)]
    for cp in copies:
        cp.start()
    return copies


def keys_kernel(lat_hbm, rot_hbm, cos_ref, sin_ref, gain_hbm, up_hbm, o_ref, lat_ref, rot_ref, gain_ref, up_ref, sems):
    pairs = ((lat_hbm, lat_ref), (gain_hbm, gain_ref), (up_hbm, up_ref), (rot_hbm, rot_ref))
    for cp in fetch(pairs, sems):
        cp.wait()
    lat = lat_ref[...].astype(F32)
    lat = (lat * lax.rsqrt(jnp.mean(lat * lat, axis=1, keepdims=True) + 1e-06) * gain_ref[...]).astype(BF)
    kv = jnp.dot(lat, up_ref[...], preferred_element_type=F32).T
    rot = turn(rot_ref[...], cos_ref[...], sin_ref[...])
    pack = jnp.concatenate([kv[:PLAIN], rot, kv[PLAIN:]], axis=0).astype(BF)
    for b in range(o_ref.shape[0]):
        o_ref[b] = pack


def rows_kernel(
    c_ref, cos_ref, sin_ref, q_hbm, tok_hbm, gain_hbm, pick_hbm, gl_hbm, il_hbm,
    q_out, o_ref, w_ref, q_ref, tok_ref, gain_ref, pick_ref, gl_ref, il_ref, sems,
):
    c = c_ref[0]
    pairs = (
        (q_hbm, q_ref), (tok_hbm, tok_ref), (gain_hbm, gain_ref), (pick_hbm, pick_ref), (gl_hbm, gl_ref), (il_hbm, il_ref)
    )
    for cp in fetch(pairs, sems):
        cp.wait()
    tok = tok_ref.shape[0]
    experts = o_ref.shape[0] // 8
    q = jnp.concatenate([q_ref[:PLAIN].astype(F32), turn(q_ref[PLAIN:], cos_ref[...], sin_ref[...])], axis=0)
    q_out[...] = q.T.astype(BF)
    vals = tok_ref[...].astype(F32)
    cen = vals - jnp.mean(vals, axis=1, keepdims=True)
    var = jnp.mean(cen * cen, axis=1, keepdims=True)
    normed = (cen * lax.rsqrt(var + 1e-05) * gain_ref[...]).astype(BF)
    eid = lax.broadcasted_iota(jnp.int32, (experts, tok), 0)
    p0, p1 = pick_ref[0:1, :], pick_ref[1:2, :]
    hit0, hit1 = eid == p0, eid == p1
    hit = hit0 | hit1
    before = lax.broadcasted_iota(jnp.int32, (tok, tok), 0) < lax.broadcasted_iota(jnp.int32, (tok, tok), 1)
    rank = jnp.dot(
        jnp.where(hit, 1.0, 0.0).astype(BF), jnp.where(before, 1.0, 0.0).astype(BF), preferred_element_type=F32
    )
    code = jnp.where(hit, rank, -1.0)
    slot = (lax.broadcasted_iota(jnp.int32, (8, tok), 0) + 8 * c).astype(F32)
    sel = jnp.concatenate([jnp.where(code[e : e + 1, :] == slot, 1.0, 0.0) for e in range(experts)], axis=0)
    o_ref[...] = jnp.dot(sel.astype(BF), normed, preferred_element_type=F32).astype(BF)
    gl = gl_ref[...]
    home = p0 // (experts // GROUPS)
    gid = lax.broadcasted_iota(jnp.int32, (GROUPS, tok), 0)
    own = jnp.sum(jnp.where(gid == home, gl, 0.0), axis=0, keepdims=True)
    share = 1.0 / jnp.sum(jnp.exp(gl - own), axis=0, keepdims=True)
    gap = il_ref[0:1, :] - il_ref[1:2, :]
    first = share * (1.0 / (1.0 + jnp.exp(-gap)))
    second = share * (1.0 / (1.0 + jnp.exp(gap)))
    weight = jnp.where(hit0, first, 0.0) + jnp.where(hit1, second, 0.0)
    spread = sel * jnp.concatenate([jnp.broadcast_to(weight[e : e + 1, :], (8, tok)) for e in range(experts)], axis=0)
    hi = spread.astype(BF).astype(F32)
    w_ref[...] = jnp.concatenate([hi, spread - hi], axis=0).T.astype(BF)


def attend_kernel(where_ref, q0, q1, q2, q3, kv_ref, o0, o1, o2, o3):
    z = where_ref[0]
    x = where_ref[1]
    zs, _, tok = kv_ref.shape
    xs = 4
    keys = jnp.concatenate([kv_ref[b, : PLAIN + ROT, :] for b in range(zs)], axis=1)
    vals = jnp.concatenate([kv_ref[b, PLAIN + ROT :, :] for b in range(zs)], axis=1)
    col = lax.broadcasted_iota(jnp.int32, (1, zs * tok), 1)
    key_seg = ((col // tok) * xs + x) * (tok // SEG) + (col % tok) // SEG
    row = lax.broadcasted_iota(jnp.int32, (tok, 1), 0)
    scale = (PLAIN + ROT) ** -0.5
    lane = lax.broadcasted_iota(jnp.int32, (tok, 128), 1)
    for k, (q_ref, o_ref) in enumerate(((q0, o0), (q1, o1), (q2, o2), (q3, o3))):
        xq = lax.rem(x + xs - k, xs)
        q_seg = (z * xs + xq) * (tok // SEG) + row // SEG
        s = jnp.dot(q_ref[...], keys, preferred_element_type=F32) * scale
        s = jnp.where(q_seg >= key_seg, s, -3e38)
        m = jnp.maximum(jnp.max(s, axis=1, keepdims=True), -1e30)
        p = jnp.exp(s - m)
        l = jnp.sum(p, axis=1, keepdims=True)
        acc = lax.dot_general(p.astype(BF), vals, (((1,), (1,)), ((), ())), preferred_element_type=F32)
        out = jnp.concatenate([acc, jnp.zeros((tok, 128 - VAL), F32)], axis=1)
        for i, piece in enumerate(split3(m) + split3(l)):
            out = jnp.where(lane == VAL + i, piece, out)
        o_ref[...] = out.astype(BF)


def mix_kernel(c_ref, a0, a1, a2, a3, w_ref, keep_ref, send_ref, res_ref):
    c = c_ref[0]
    parts = [r[...].astype(F32) for r in (a0, a1, a2, a3)]
    ms = [p[:, VAL : VAL + 1] + p[:, VAL + 1 : VAL + 2] + p[:, VAL + 2 : VAL + 3] for p in parts]
    ls = [p[:, VAL + 3 : VAL + 4] + p[:, VAL + 4 : VAL + 5] + p[:, VAL + 5 : VAL + 6] for p in parts]
    m = functools.reduce(jnp.maximum, ms)
    total = 0.0
    denom = 0.0
    for p, mp, lp in zip(parts, ms, ls):
        w = jnp.exp(mp - m)
        total = total + w * p[:, :VAL]
        denom = denom + w * lp
    attended = (total / denom).astype(BF)
    res_ref[...] = jnp.dot(attended, w_ref[...], preferred_element_type=F32)
    for y in range(keep_ref.shape[0]):
        keep_ref[y] = res_ref[pl.ds(pl.multiple_of(16 * y + 8 * c, 8), 8), :].astype(BF)
        send_ref[y] = res_ref[pl.ds(pl.multiple_of(16 * y + 8 * (1 - c), 8), 8), :].astype(BF)


def ffn_kernel(x_ref, g0h, u0h, d0h, g1h, u1h, d1h, o_ref, g0, u0, d0, g1, u1, d1, sems):
    cps = fetch(((g0h, g0), (u0h, u0), (d0h, d0), (g1h, g1), (u1h, u1), (d1h, d1)), sems)
    rows = x_ref[...]
    acc = None
    for i, (g_ref, u_ref, d_ref) in enumerate(((g0, u0, d0), (g1, u1, d1))):
        cps[3 * i].wait()
        g = jnp.dot(rows, g_ref[...], preferred_element_type=F32)
        cps[3 * i + 1].wait()
        u = jnp.dot(rows, u_ref[...], preferred_element_type=F32)
        h = (g / (1.0 + jnp.exp(-g)) * u).astype(BF)
        cps[3 * i + 2].wait()
        part = jnp.dot(h, d_ref[...], preferred_element_type=F32)
        acc = part if acc is None else acc + part
    o_ref[...] = acc.astype(BF)


def combine_kernel(c_ref, r_ref, w_ref, keep_ref, send_ref):
    c = c_ref[0]
    for i, o_ref in ((c, keep_ref), (1 - c, send_ref)):
        cols = jnp.concatenate(
            [r_ref[:, pl.ds(pl.multiple_of(128 * (2 * y + i), 128), 128)] for y in range(o_ref.shape[0])], axis=1
        )
        both = jnp.concatenate([cols, cols], axis=0)
        out = jnp.dot(w_ref[...], both, preferred_element_type=F32)
        for y in range(o_ref.shape[0]):
            o_ref[y] = out[:, 128 * y : 128 * (y + 1)].astype(o_ref.dtype)


def vm(n):
    return [pl.BlockSpec(memory_space=pltpu.VMEM)] * n


def hb(n):
    return [pl.BlockSpec(memory_space=pltpu.HBM)] * n


SM = [pl.BlockSpec(memory_space=pltpu.SMEM)]


def call(kernel, name, outs, ins, mib, scratch=()):
    return pl.pallas_call(
        kernel,
        out_shape=[jax.ShapeDtypeStruct(shape, dtype) for shape, dtype in outs],
        in_specs=ins,
        out_specs=vm(len(outs)),
        scratch_shapes=list(scratch),
        name=name,
        compiler_params=pltpu.CompilerParams(vmem_limit_bytes=mib * MIB),
    )


def per_device(
    queries, token_latents, key_rotary, latent_norm_gain, latent_up_weight, w_out,
    tokens_b, moe_gain, group_logits, inner_logits, expert_pick, w_gate, w_up, w_down,
):
    ep = ("z", "x")
    zs, xs, ys = lax.axis_size("z"), lax.axis_size("x"), lax.axis_size("y")
    z, x, c = (lax.axis_index(n).astype(jnp.int32) for n in ("z", "x", "c"))
    tok = queries.shape[0]
    width = tokens_b.shape[1]
    experts = zs * xs
    half = 8
    slots = experts * half
    ff = w_gate.shape[2]
    swap = [(0, 1), (1, 0)]

    positions = ((z * xs + x) * tok + jnp.arange(tok, dtype=jnp.int32)).astype(F32)
    freq = jnp.power(10000.0, -jnp.arange(ROT // 2, dtype=F32) * 2.0 / ROT)
    ang = freq[:, None] * positions[None, :]
    cos, sin = jnp.cos(ang), jnp.sin(ang)

    lat_w = token_latents.shape[1]
    (pack,) = call(
        keys_kernel, "keys", [((zs, PLAIN + ROT + VAL, tok), BF)], hb(2) + vm(2) + hb(2), 16,
        [
            pltpu.VMEM((tok, lat_w), BF), pltpu.VMEM((ROT, tok), BF), pltpu.VMEM((1, lat_w), F32),
            pltpu.VMEM((lat_w, PLAIN + VAL), BF), pltpu.SemaphoreType.DMA((4,)),
        ],
    )(
        token_latents, key_rotary.T, cos, sin, latent_norm_gain[None, :], latent_up_weight
    )
    kv_all = lax.all_to_all(pack, "z", 0, 0, tiled=True)

    cs = c.reshape(1)
    q_own, outbound, spread = call(
        rows_kernel, "rows",
        [((tok, PLAIN + ROT), BF), ((slots, width), BF), ((tok, 2 * slots), BF)], SM + vm(2) + hb(6), 24,
        [
            pltpu.VMEM((PLAIN + ROT, tok), BF), pltpu.VMEM((tok, width), BF), pltpu.VMEM((1, width), F32),
            pltpu.VMEM((2, tok), jnp.int32), pltpu.VMEM((GROUPS, tok), F32), pltpu.VMEM((2, tok), F32),
            pltpu.SemaphoreType.DMA((6,)),
        ],
    )(cs, cos, sin, queries.T, tokens_b, moe_gain[None, :], expert_pick.T, group_logits.T, inner_logits.T)
    qs = [q_own] + [
        lax.ppermute(q_own, "x", [(i, (i + k) % xs) for i in range(xs)]) for k in range(1, xs)
    ]
    outbound, kv_all, qs = lax.optimization_barrier((outbound, kv_all, qs))
    arrived = lax.all_to_all(outbound.reshape(experts, half, width), ep, 0, 0, tiled=True)

    wg, wu, wd = w_gate[0], w_up[0], w_down[0]
    wg2, wu2, wd2 = (lax.ppermute(w, "c", swap) for w in (wg, wu, wd))

    parts = call(attend_kernel, "attend", [((tok, 128), BF)] * xs, SM + vm(5), 16)(
        jnp.stack([z, x]), *qs, kv_all
    )
    back = [parts[0]] + [
        lax.ppermute(parts[k], "x", [(i, (i - k) % xs) for i in range(xs)]) for k in range(1, xs)
    ]
    keep_mix, send_mix = call(
        mix_kernel, "mix", [((ys, 8, width), BF)] * 2, SM + vm(5), 16, [pltpu.VMEM((tok, width), F32)]
    )(cs, *back, w_out)

    arrived, keep_mix, send_mix = lax.optimization_barrier((arrived, keep_mix, send_mix))
    into, outof = pltpu.VMEM((width, ff), BF), pltpu.VMEM((ff, width), BF)
    (result,) = call(
        ffn_kernel, "ffn", [((slots, width), BF)], vm(1) + hb(6), 32,
        [into, into, outof, into, into, outof, pltpu.SemaphoreType.DMA((6,))],
    )(arrived.reshape(slots, width), wg, wu, wd, wg2, wu2, wd2)
    returned = lax.all_to_all(result.reshape(experts, half, width), ep, 0, 0, tiled=True)
    got_mix = lax.ppermute(send_mix, "c", swap)
    mix_half = (keep_mix.astype(F32) + got_mix.astype(F32)).astype(BF)
    mix_rows = mix_half.reshape(ys, 8, width // 128, 128).transpose(0, 2, 1, 3).reshape(ys, width // 16, 128)

    returned, mix_rows = lax.optimization_barrier((returned, mix_rows))
    keep, send = call(
        combine_kernel, "combine", [((ys, tok, 128), F32), ((ys, tok, 128), BF)], SM + vm(2), 16
    )(cs, returned.reshape(slots, width), spread)
    got = lax.ppermute(send, "c", swap)
    moe_half = (keep + got.astype(F32)).astype(BF)
    last = lax.all_to_all(jnp.concatenate([moe_half, mix_rows], axis=1), "y", 0, 0, tiled=True)
    summed = jnp.sum(last.astype(F32), axis=0).astype(BF)
    expert_out = summed[:tok]
    mixer_out = summed[tok:].reshape(width // 128, 8, 128).transpose(1, 0, 2).reshape(8, width)
    return mixer_out, expert_out


def solution(mesh):
    fine = Mesh(mesh.devices.reshape(8, 4, 8, 2), ("z", "x", "y", "c"))
    e, t = ("z", "x"), ("y", "c")
    in_specs = (
        P(e, t), P(e, None), P(e, None), P(), P(None, t), P(t, None), P(e, None), P(),
        P(e, None), P(e, None), P(e, None), P(e, None, t), P(e, None, t), P(e, t, None),
    )
    out_specs = (P(e + t, None), P(e, t))
    return jax.shard_map(per_device, mesh=fine, in_specs=in_specs, out_specs=out_specs, check_vma=False)
```

```python
import functools

import jax
import jax.numpy as jnp
from jax import lax
from jax.experimental import pallas as pl
from jax.experimental.pallas import tpu as pltpu
from jax.sharding import Mesh, PartitionSpec as P

PLAIN = 64
ROT = 32
VAL = 64
SEG = 64
GROUPS = 4
BF = jnp.bfloat16
F32 = jnp.float32
MIB = 1024 * 1024


def turn(v, cos, sin):
    a, b = v[: ROT // 2].astype(F32), v[ROT // 2 :].astype(F32)
    return jnp.concatenate([a * cos - b * sin, b * cos + a * sin], axis=0)


def fetch(pairs, sems):
    copies = [pltpu.make_async_copy(src, dst, sems.at[i]) for i, (src, dst) in enumerate(pairs)]
    for cp in copies:
        cp.start()
    return copies


def choose(c, pick_ref, experts):
    tok = pick_ref.shape[1]
    eid = lax.broadcasted_iota(jnp.int32, (experts, tok), 0)
    hit0, hit1 = eid == pick_ref[0:1, :], eid == pick_ref[1:2, :]
    hit = hit0 | hit1
    before = lax.broadcasted_iota(jnp.int32, (tok, tok), 0) < lax.broadcasted_iota(jnp.int32, (tok, tok), 1)
    rank = jnp.dot(
        jnp.where(hit, 1.0, 0.0).astype(BF), jnp.where(before, 1.0, 0.0).astype(BF), preferred_element_type=F32
    )
    code = jnp.where(hit, rank, -1.0)
    slot = (lax.broadcasted_iota(jnp.int32, (8, tok), 0) + 8 * c).astype(F32)
    sel = jnp.concatenate([jnp.where(code[e : e + 1, :] == slot, 1.0, 0.0) for e in range(experts)], axis=0)
    return hit0, hit1, sel


def keys_kernel(
    c_ref, lat_hbm, rot_hbm, cos_ref, sin_ref, gain_hbm, up_hbm, pick_hbm, gl_hbm, il_hbm,
    o_ref, w_ref, lat_ref, rot_ref, gain_ref, up_ref, pick_ref, gl_ref, il_ref, sems,
):
    pairs = (
        (lat_hbm, lat_ref), (gain_hbm, gain_ref), (up_hbm, up_ref), (rot_hbm, rot_ref),
        (pick_hbm, pick_ref), (gl_hbm, gl_ref), (il_hbm, il_ref),
    )
    for cp in fetch(pairs, sems):
        cp.wait()
    lat = lat_ref[...].astype(F32)
    lat = (lat * lax.rsqrt(jnp.mean(lat * lat, axis=1, keepdims=True) + 1e-06) * gain_ref[...]).astype(BF)
    kv = jnp.dot(lat, up_ref[...], preferred_element_type=F32).T
    rot = turn(rot_ref[...], cos_ref[...], sin_ref[...])
    pack = jnp.concatenate([kv[:PLAIN], rot, kv[PLAIN:]], axis=0).astype(BF)
    for b in range(o_ref.shape[0]):
        o_ref[b] = pack

    experts = w_ref.shape[1] // 16
    tok = w_ref.shape[0]
    hit0, hit1, sel = choose(c_ref[0], pick_ref, experts)
    gl = gl_ref[...]
    home = pick_ref[0:1, :] // (experts // GROUPS)
    gid = lax.broadcasted_iota(jnp.int32, (GROUPS, tok), 0)
    own = jnp.sum(jnp.where(gid == home, gl, 0.0), axis=0, keepdims=True)
    share = 1.0 / jnp.sum(jnp.exp(gl - own), axis=0, keepdims=True)
    gap = il_ref[0:1, :] - il_ref[1:2, :]
    first = share * (1.0 / (1.0 + jnp.exp(-gap)))
    second = share * (1.0 / (1.0 + jnp.exp(gap)))
    weight = jnp.where(hit0, first, 0.0) + jnp.where(hit1, second, 0.0)
    spread = sel * jnp.concatenate([jnp.broadcast_to(weight[e : e + 1, :], (8, tok)) for e in range(experts)], axis=0)
    hi = spread.astype(BF).astype(F32)
    w_ref[...] = jnp.concatenate([hi, spread - hi], axis=0).T.astype(BF)


def rows_kernel(c_ref, tok_hbm, gain_hbm, pick_hbm, o_ref, tok_ref, gain_ref, pick_ref, sems):
    cps = fetch(((pick_hbm, pick_ref), (tok_hbm, tok_ref), (gain_hbm, gain_ref)), sems)
    cps[0].wait()
    _, _, sel = choose(c_ref[0], pick_ref, o_ref.shape[0] // 8)
    cps[1].wait()
    cps[2].wait()
    vals = tok_ref[...].astype(F32)
    cen = vals - jnp.mean(vals, axis=1, keepdims=True)
    var = jnp.mean(cen * cen, axis=1, keepdims=True)
    normed = (cen * lax.rsqrt(var + 1e-05) * gain_ref[...]).astype(BF)
    o_ref[...] = jnp.dot(sel.astype(BF), normed, preferred_element_type=F32).astype(BF)


def mixer_kernel(where_ref, q_ref, cos_ref, sin_ref, kv0, kv1, kv2, kv3, w_ref, keep_ref, send_ref, res_ref):
    z, x, c = where_ref[0], where_ref[1], where_ref[2]
    kvs = (kv0, kv1, kv2, kv3)
    xs = len(kvs)
    zs, _, tok = kv0.shape
    segs = tok // SEG
    q = jnp.concatenate([q_ref[:PLAIN].astype(F32), turn(q_ref[PLAIN:], cos_ref[...], sin_ref[...])], axis=0)
    q = q.T.astype(BF)
    col = lax.broadcasted_iota(jnp.int32, (1, zs * tok), 1)
    row = lax.broadcasted_iota(jnp.int32, (tok, 1), 0)
    q_seg = (z * xs + x) * segs + row // SEG
    scale = (PLAIN + ROT) ** -0.5
    scores, top = [], None
    for k, kv in enumerate(kvs):
        keys = jnp.concatenate([kv[b, : PLAIN + ROT, :] for b in range(zs)], axis=1)
        xk = lax.rem(x + xs - k, xs)
        key_seg = ((col // tok) * xs + xk) * segs + (col % tok) // SEG
        s = jnp.dot(q, keys, preferred_element_type=F32) * scale
        s = jnp.where(q_seg >= key_seg, s, -3e38)
        m = jnp.max(s, axis=1, keepdims=True)
        top = m if top is None else jnp.maximum(top, m)
        scores.append(s)
    total = denom = 0.0
    for s, kv in zip(scores, kvs):
        vals = jnp.concatenate([kv[b, PLAIN + ROT :, :] for b in range(zs)], axis=1)
        p = jnp.exp(s - top)
        denom = denom + jnp.sum(p, axis=1, keepdims=True)
        total = total + lax.dot_general(p.astype(BF), vals, (((1,), (1,)), ((), ())), preferred_element_type=F32)
    attended = (total / denom).astype(BF)
    res_ref[...] = jnp.dot(attended, w_ref[...], preferred_element_type=F32)
    for y in range(keep_ref.shape[0]):
        keep_ref[y] = res_ref[pl.ds(pl.multiple_of(16 * y + 8 * c, 8), 8), :].astype(BF)
        send_ref[y] = res_ref[pl.ds(pl.multiple_of(16 * y + 8 * (1 - c), 8), 8), :].astype(BF)


def ffn_kernel(x_ref, g0h, u0h, d0h, g1h, u1h, d1h, o_ref, gu0, gu1, d0, d1, sems):
    f = d0.shape[0]
    cps = fetch((
        (g0h, gu0.at[:, :f]), (u0h, gu0.at[:, f:]), (g1h, gu1.at[:, :f]), (u1h, gu1.at[:, f:]), (d0h, d0), (d1h, d1)
    ), sems)
    rows = x_ref[...]
    hs = []
    for i, gu_ref in enumerate((gu0, gu1)):
        cps[2 * i].wait()
        cps[2 * i + 1].wait()
        both = jnp.dot(rows, gu_ref[...], preferred_element_type=F32)
        g, u = both[:, :f], both[:, f:]
        hs.append((g / (1.0 + jnp.exp(-g)) * u).astype(BF))
    cps[4].wait()
    cps[5].wait()
    acc = jnp.dot(hs[0], d0[...], preferred_element_type=F32) + jnp.dot(hs[1], d1[...], preferred_element_type=F32)
    o_ref[...] = acc.astype(BF)


def combine_kernel(c_ref, r_ref, w_ref, keep_ref, send_ref):
    c = c_ref[0]
    for i, o_ref in ((c, keep_ref), (1 - c, send_ref)):
        cols = jnp.concatenate(
            [r_ref[:, pl.ds(pl.multiple_of(128 * (2 * y + i), 128), 128)] for y in range(o_ref.shape[0])], axis=1
        )
        both = jnp.concatenate([cols, cols], axis=0)
        out = jnp.dot(w_ref[...], both, preferred_element_type=F32)
        for y in range(o_ref.shape[0]):
            o_ref[y] = out[:, 128 * y : 128 * (y + 1)].astype(o_ref.dtype)


def vm(n):
    return [pl.BlockSpec(memory_space=pltpu.VMEM)] * n


def hb(n):
    return [pl.BlockSpec(memory_space=pltpu.HBM)] * n


SM = [pl.BlockSpec(memory_space=pltpu.SMEM)]


def call(kernel, name, outs, ins, mib, scratch=()):
    return pl.pallas_call(
        kernel,
        out_shape=[jax.ShapeDtypeStruct(shape, dtype) for shape, dtype in outs],
        in_specs=ins,
        out_specs=vm(len(outs)),
        scratch_shapes=list(scratch),
        cost_estimate=pl.CostEstimate(flops=1000000, bytes_accessed=0, transcendentals=0),
        name=name,
        compiler_params=pltpu.CompilerParams(vmem_limit_bytes=mib * MIB),
    )


def per_device(
    queries, token_latents, key_rotary, latent_norm_gain, latent_up_weight, w_out,
    tokens_b, moe_gain, group_logits, inner_logits, expert_pick, w_gate, w_up, w_down,
):
    ep = ("z", "x")
    zs, xs, ys = lax.axis_size("z"), lax.axis_size("x"), lax.axis_size("y")
    z, x, c = (lax.axis_index(n).astype(jnp.int32) for n in ("z", "x", "c"))
    tok = queries.shape[0]
    width = tokens_b.shape[1]
    experts = zs * xs
    half = 8
    slots = experts * half
    ff = w_gate.shape[2]
    swap = [(0, 1), (1, 0)]

    positions = ((z * xs + x) * tok + jnp.arange(tok, dtype=jnp.int32)).astype(F32)
    freq = jnp.power(10000.0, -jnp.arange(ROT // 2, dtype=F32) * 2.0 / ROT)
    ang = freq[:, None] * positions[None, :]
    cos, sin = jnp.cos(ang), jnp.sin(ang)

    where = jnp.stack([z, x, c])
    cs = c.reshape(1)
    (outbound,) = call(
        rows_kernel, "rows", [((slots, width), BF)], SM + hb(3), 24,
        [
            pltpu.VMEM((tok, width), BF), pltpu.VMEM((1, width), F32), pltpu.VMEM((2, tok), jnp.int32),
            pltpu.SemaphoreType.DMA((3,)),
        ],
    )(cs, tokens_b, moe_gain[None, :], expert_pick.T)
    arrived = lax.all_to_all(outbound.reshape(experts, half, width), ep, 0, 0, tiled=True)

    wg, wu, wd = w_gate[0], w_up[0], w_down[0]
    wg2, wu2, wd2 = (lax.ppermute(w, "c", swap) for w in (wg, wu, wd))

    lat_w = token_latents.shape[1]
    pack, spread = call(
        keys_kernel, "keys", [((zs, PLAIN + ROT + VAL, tok), BF), ((tok, 2 * slots), BF)],
        SM + hb(2) + vm(2) + hb(5), 16,
        [
            pltpu.VMEM((tok, lat_w), BF), pltpu.VMEM((ROT, tok), BF), pltpu.VMEM((1, lat_w), F32),
            pltpu.VMEM((lat_w, PLAIN + VAL), BF), pltpu.VMEM((2, tok), jnp.int32),
            pltpu.VMEM((GROUPS, tok), F32), pltpu.VMEM((2, tok), F32), pltpu.SemaphoreType.DMA((7,)),
        ],
    )(
        cs, token_latents, key_rotary.T, cos, sin, latent_norm_gain[None, :], latent_up_weight,
        expert_pick.T, group_logits.T, inner_logits.T,
    )
    arrived, pack = lax.optimization_barrier((arrived, pack))
    kv_all = lax.all_to_all(pack, "z", 0, 0, tiled=True)
    into, outof = pltpu.VMEM((width, 2 * ff), BF), pltpu.VMEM((ff, width), BF)
    (result,) = call(
        ffn_kernel, "ffn", [((slots, width), BF)], vm(1) + hb(6), 32,
        [into, into, outof, outof, pltpu.SemaphoreType.DMA((6,))],
    )(arrived.reshape(slots, width), wg, wu, wd, wg2, wu2, wd2)
    result, kv_all = lax.optimization_barrier((result, kv_all))
    returned = lax.all_to_all(result.reshape(experts, half, width), ep, 0, 0, tiled=True)
    kvs = [kv_all] + [
        lax.ppermute(kv_all, "x", [(i, (i + k) % xs) for i in range(xs)]) for k in (1, 3, 2)
    ]
    kvs = [kvs[0], kvs[1], kvs[3], kvs[2]]
    keep_mix, send_mix = call(
        mixer_kernel, "mixer", [((ys, 8, width), BF)] * 2, SM + vm(8), 24, [pltpu.VMEM((tok, width), F32)]
    )(where, queries.T, cos, sin, *kvs, w_out)
    got_mix = lax.ppermute(send_mix, "c", swap)
    mix_half = (keep_mix.astype(F32) + got_mix.astype(F32)).astype(BF)
    mix_rows = mix_half.reshape(ys, 8, width // 128, 128).transpose(0, 2, 1, 3).reshape(ys, width // 16, 128)

    returned, mix_rows = lax.optimization_barrier((returned, mix_rows))
    keep, send = call(
        combine_kernel, "combine", [((ys, tok, 128), F32), ((ys, tok, 128), BF)], SM + vm(2), 16
    )(cs, returned.reshape(slots, width), spread)
    got = lax.ppermute(send, "c", swap)
    moe_half = (keep + got.astype(F32)).astype(BF)
    last = lax.all_to_all(jnp.concatenate([moe_half, mix_rows], axis=1), "y", 0, 0, tiled=True)
    summed = jnp.sum(last.astype(F32), axis=0).astype(BF)
    expert_out = summed[:tok]
    mixer_out = summed[tok:].reshape(width // 128, 8, 128).transpose(1, 0, 2).reshape(8, width)
    return mixer_out, expert_out


def solution(mesh):
    fine = Mesh(mesh.devices.reshape(8, 4, 8, 2), ("z", "x", "y", "c"))
    e, t = ("z", "x"), ("y", "c")
    in_specs = (
        P(e, t), P(e, None), P(e, None), P(), P(None, t), P(t, None), P(e, None), P(),
        P(e, None), P(e, None), P(e, None), P(e, None, t), P(e, None, t), P(e, t, None),
    )
    out_specs = (P(e + t, None), P(e, t))
    return jax.shard_map(per_device, mesh=fine, in_specs=in_specs, out_specs=out_specs, check_vma=False)
```

```python
import functools

import jax
import jax.numpy as jnp
from jax import lax
from jax.experimental import pallas as pl
from jax.experimental.pallas import tpu as pltpu
from jax.sharding import Mesh, PartitionSpec as P

PLAIN = 64
ROT = 32
VAL = 64
SEG = 64
GROUPS = 4
BF = jnp.bfloat16
F32 = jnp.float32
MIB = 1024 * 1024


def turn(v, cos, sin):
    a, b = v[: ROT // 2].astype(F32), v[ROT // 2 :].astype(F32)
    return jnp.concatenate([a * cos - b * sin, b * cos + a * sin], axis=0)


def fetch(pairs, sems):
    copies = [pltpu.make_async_copy(src, dst, sems.at[i]) for i, (src, dst) in enumerate(pairs)]
    for cp in copies:
        cp.start()
    return copies


def choose(c, pick_ref, experts):
    tok = pick_ref.shape[1]
    eid = lax.broadcasted_iota(jnp.int32, (experts, tok), 0)
    hit0, hit1 = eid == pick_ref[0:1, :], eid == pick_ref[1:2, :]
    hit = hit0 | hit1
    before = lax.broadcasted_iota(jnp.int32, (tok, tok), 0) < lax.broadcasted_iota(jnp.int32, (tok, tok), 1)
    rank = jnp.dot(
        jnp.where(hit, 1.0, 0.0).astype(BF), jnp.where(before, 1.0, 0.0).astype(BF), preferred_element_type=F32
    )
    code = jnp.where(hit, rank, -1.0)
    slot = (lax.broadcasted_iota(jnp.int32, (8, tok), 0) + 8 * c).astype(F32)
    sel = jnp.concatenate([jnp.where(code[e : e + 1, :] == slot, 1.0, 0.0) for e in range(experts)], axis=0)
    return hit0, hit1, sel


def keys_kernel(
    c_ref, lat_hbm, rot_hbm, cos_ref, sin_ref, gain_hbm, up_hbm, pick_hbm, gl_hbm, il_hbm,
    o_ref, w_ref, lat_ref, rot_ref, gain_ref, up_ref, pick_ref, gl_ref, il_ref, sems,
):
    pairs = (
        (lat_hbm, lat_ref), (gain_hbm, gain_ref), (up_hbm, up_ref), (rot_hbm, rot_ref),
        (pick_hbm, pick_ref), (gl_hbm, gl_ref), (il_hbm, il_ref),
    )
    for cp in fetch(pairs, sems):
        cp.wait()
    lat = lat_ref[...].astype(F32)
    lat = (lat * lax.rsqrt(jnp.mean(lat * lat, axis=1, keepdims=True) + 1e-06) * gain_ref[...]).astype(BF)
    kv = jnp.dot(lat, up_ref[...], preferred_element_type=F32).T
    rot = turn(rot_ref[...], cos_ref[...], sin_ref[...])
    pack = jnp.concatenate([kv[:PLAIN], rot, kv[PLAIN:]], axis=0).astype(BF)
    for b in range(o_ref.shape[0]):
        o_ref[b] = pack

    experts = w_ref.shape[1] // 16
    tok = w_ref.shape[0]
    hit0, hit1, sel = choose(c_ref[0], pick_ref, experts)
    gl = gl_ref[...]
    home = pick_ref[0:1, :] // (experts // GROUPS)
    gid = lax.broadcasted_iota(jnp.int32, (GROUPS, tok), 0)
    own = jnp.sum(jnp.where(gid == home, gl, 0.0), axis=0, keepdims=True)
    share = 1.0 / jnp.sum(jnp.exp(gl - own), axis=0, keepdims=True)
    gap = il_ref[0:1, :] - il_ref[1:2, :]
    first = share * (1.0 / (1.0 + jnp.exp(-gap)))
    second = share * (1.0 / (1.0 + jnp.exp(gap)))
    weight = jnp.where(hit0, first, 0.0) + jnp.where(hit1, second, 0.0)
    spread = sel * jnp.concatenate([jnp.broadcast_to(weight[e : e + 1, :], (8, tok)) for e in range(experts)], axis=0)
    hi = spread.astype(BF).astype(F32)
    w_ref[...] = jnp.concatenate([hi, spread - hi], axis=0).T.astype(BF)


def rows_kernel(c_ref, tok_hbm, gain_hbm, pick_hbm, o_ref, tok_ref, gain_ref, pick_ref, sems):
    cps = fetch(((pick_hbm, pick_ref), (tok_hbm, tok_ref), (gain_hbm, gain_ref)), sems)
    cps[0].wait()
    _, _, sel = choose(c_ref[0], pick_ref, o_ref.shape[0] // 8)
    cps[1].wait()
    cps[2].wait()
    vals = tok_ref[...].astype(F32)
    cen = vals - jnp.mean(vals, axis=1, keepdims=True)
    var = jnp.mean(cen * cen, axis=1, keepdims=True)
    normed = (cen * lax.rsqrt(var + 1e-05) * gain_ref[...]).astype(BF)
    o_ref[...] = jnp.dot(sel.astype(BF), normed, preferred_element_type=F32).astype(BF)


def split3(v):
    hi = v.astype(BF).astype(F32)
    rest = v - hi
    mid = rest.astype(BF).astype(F32)
    return hi, mid, rest - mid


def query_kernel(q_ref, cos_ref, sin_ref, o_ref):
    q = jnp.concatenate([q_ref[:PLAIN].astype(F32), turn(q_ref[PLAIN:], cos_ref[...], sin_ref[...])], axis=0)
    o_ref[...] = q.T.astype(BF)


def attend_kernel(where_ref, q0, q1, kv0, kv1, o0, o1):
    z, x = where_ref[0], where_ref[1]
    xs = 4
    zs, _, tok = kv0.shape
    segs = tok // SEG
    kvs = (kv0, kv1)
    keys = jnp.concatenate([kv[b, : PLAIN + ROT, :] for kv in kvs for b in range(zs)], axis=1)
    vals = jnp.concatenate([kv[b, PLAIN + ROT :, :] for kv in kvs for b in range(zs)], axis=1)
    col = lax.broadcasted_iota(jnp.int32, (1, 2 * zs * tok), 1)
    xk = jnp.where(col < zs * tok, x, lax.bitwise_xor(x, 1))
    key_seg = (((col // tok) % zs) * xs + xk) * segs + (col % tok) // SEG
    row = lax.broadcasted_iota(jnp.int32, (tok, 1), 0)
    scale = (PLAIN + ROT) ** -0.5
    lane = lax.broadcasted_iota(jnp.int32, (tok, 128), 1)
    for q_ref, o_ref, xq in ((q1, o1, lax.bitwise_xor(x, 2)), (q0, o0, x)):
        q_seg = (z * xs + xq) * segs + row // SEG
        s = jnp.dot(q_ref[...], keys, preferred_element_type=F32) * scale
        s = jnp.where(q_seg >= key_seg, s, -3e38)
        m = jnp.maximum(jnp.max(s, axis=1, keepdims=True), -1e30)
        p = jnp.exp(s - m)
        l = jnp.sum(p, axis=1, keepdims=True)
        acc = lax.dot_general(p.astype(BF), vals, (((1,), (1,)), ((), ())), preferred_element_type=F32)
        out = jnp.concatenate([acc, jnp.zeros((tok, 128 - VAL), F32)], axis=1)
        for i, piece in enumerate(split3(m) + split3(l)):
            out = jnp.where(lane == VAL + i, piece, out)
        o_ref[...] = out.astype(BF)


def mix_kernel(where_ref, a0, a1, w_ref, keep_ref, send_ref, res_ref):
    c = where_ref[2]
    parts = [r[...].astype(F32) for r in (a0, a1)]
    ms = [p[:, VAL : VAL + 1] + p[:, VAL + 1 : VAL + 2] + p[:, VAL + 2 : VAL + 3] for p in parts]
    ls = [p[:, VAL + 3 : VAL + 4] + p[:, VAL + 4 : VAL + 5] + p[:, VAL + 5 : VAL + 6] for p in parts]
    m = functools.reduce(jnp.maximum, ms)
    total = denom = 0.0
    for p, mp, lp in zip(parts, ms, ls):
        w = jnp.exp(mp - m)
        total = total + w * p[:, :VAL]
        denom = denom + w * lp
    attended = (total / denom).astype(BF)
    res_ref[...] = jnp.dot(attended, w_ref[...], preferred_element_type=F32)
    for y in range(keep_ref.shape[0]):
        keep_ref[y] = res_ref[pl.ds(pl.multiple_of(16 * y + 8 * c, 8), 8), :].astype(BF)
        send_ref[y] = res_ref[pl.ds(pl.multiple_of(16 * y + 8 * (1 - c), 8), 8), :].astype(BF)


def ffn_kernel(x_ref, g0h, u0h, d0h, g1h, u1h, d1h, o_ref, gu0, gu1, d0, d1, sems):
    f = d0.shape[0]
    cps = fetch((
        (g0h, gu0.at[:, :f]), (u0h, gu0.at[:, f:]), (g1h, gu1.at[:, :f]), (u1h, gu1.at[:, f:]), (d0h, d0), (d1h, d1)
    ), sems)
    rows = x_ref[...]
    hs = []
    for i, gu_ref in enumerate((gu0, gu1)):
        cps[2 * i].wait()
        cps[2 * i + 1].wait()
        both = jnp.dot(rows, gu_ref[...], preferred_element_type=F32)
        g, u = both[:, :f], both[:, f:]
        hs.append((g / (1.0 + jnp.exp(-g)) * u).astype(BF))
    cps[4].wait()
    cps[5].wait()
    acc = jnp.dot(hs[0], d0[...], preferred_element_type=F32) + jnp.dot(hs[1], d1[...], preferred_element_type=F32)
    o_ref[...] = acc.astype(BF)


def combine_kernel(c_ref, r_ref, w_ref, keep_ref, send_ref):
    c = c_ref[0]
    for i, o_ref in ((c, keep_ref), (1 - c, send_ref)):
        cols = jnp.concatenate(
            [r_ref[:, pl.ds(pl.multiple_of(128 * (2 * y + i), 128), 128)] for y in range(o_ref.shape[0])], axis=1
        )
        both = jnp.concatenate([cols, cols], axis=0)
        out = jnp.dot(w_ref[...], both, preferred_element_type=F32)
        for y in range(o_ref.shape[0]):
            o_ref[y] = out[:, 128 * y : 128 * (y + 1)].astype(o_ref.dtype)


def vm(n):
    return [pl.BlockSpec(memory_space=pltpu.VMEM)] * n


def hb(n):
    return [pl.BlockSpec(memory_space=pltpu.HBM)] * n


SM = [pl.BlockSpec(memory_space=pltpu.SMEM)]


def call(kernel, name, outs, ins, mib, scratch=()):
    return pl.pallas_call(
        kernel,
        out_shape=[jax.ShapeDtypeStruct(shape, dtype) for shape, dtype in outs],
        in_specs=ins,
        out_specs=vm(len(outs)),
        scratch_shapes=list(scratch),
        cost_estimate=pl.CostEstimate(flops=1000000, bytes_accessed=0, transcendentals=0),
        name=name,
        compiler_params=pltpu.CompilerParams(vmem_limit_bytes=mib * MIB),
    )


def per_device(
    queries, token_latents, key_rotary, latent_norm_gain, latent_up_weight, w_out,
    tokens_b, moe_gain, group_logits, inner_logits, expert_pick, w_gate, w_up, w_down,
):
    ep = ("z", "x")
    zs, xs, ys = lax.axis_size("z"), lax.axis_size("x"), lax.axis_size("y")
    z, x, c = (lax.axis_index(n).astype(jnp.int32) for n in ("z", "x", "c"))
    tok = queries.shape[0]
    width = tokens_b.shape[1]
    experts = zs * xs
    half = 8
    slots = experts * half
    ff = w_gate.shape[2]
    swap = [(0, 1), (1, 0)]

    positions = ((z * xs + x) * tok + jnp.arange(tok, dtype=jnp.int32)).astype(F32)
    freq = jnp.power(10000.0, -jnp.arange(ROT // 2, dtype=F32) * 2.0 / ROT)
    ang = freq[:, None] * positions[None, :]
    cos, sin = jnp.cos(ang), jnp.sin(ang)

    where = jnp.stack([z, x, c])
    cs = c.reshape(1)
    (outbound,) = call(
        rows_kernel, "rows", [((slots, width), BF)], SM + hb(3), 24,
        [
            pltpu.VMEM((tok, width), BF), pltpu.VMEM((1, width), F32), pltpu.VMEM((2, tok), jnp.int32),
            pltpu.SemaphoreType.DMA((3,)),
        ],
    )(cs, tokens_b, moe_gain[None, :], expert_pick.T)
    arrived = lax.all_to_all(outbound.reshape(experts, half, width), ep, 0, 0, tiled=True)

    wg, wu, wd = w_gate[0], w_up[0], w_down[0]
    wg2, wu2, wd2 = (lax.ppermute(w, "c", swap) for w in (wg, wu, wd))

    lat_w = token_latents.shape[1]
    pack, spread = call(
        keys_kernel, "keys", [((zs, PLAIN + ROT + VAL, tok), BF), ((tok, 2 * slots), BF)],
        SM + hb(2) + vm(2) + hb(5), 16,
        [
            pltpu.VMEM((tok, lat_w), BF), pltpu.VMEM((ROT, tok), BF), pltpu.VMEM((1, lat_w), F32),
            pltpu.VMEM((lat_w, PLAIN + VAL), BF), pltpu.VMEM((2, tok), jnp.int32),
            pltpu.VMEM((GROUPS, tok), F32), pltpu.VMEM((2, tok), F32), pltpu.SemaphoreType.DMA((7,)),
        ],
    )(
        cs, token_latents, key_rotary.T, cos, sin, latent_norm_gain[None, :], latent_up_weight,
        expert_pick.T, group_logits.T, inner_logits.T,
    )
    (q_own,) = call(query_kernel, "query", [((tok, PLAIN + ROT), BF)], vm(3), 16)(queries.T, cos, sin)
    q_far = lax.ppermute(q_own, "x", [(i, i ^ 2) for i in range(xs)])
    arrived, pack, q_own, q_far = lax.optimization_barrier((arrived, pack, q_own, q_far))
    kv_all = lax.all_to_all(pack, "z", 0, 0, tiled=True)
    into, outof = pltpu.VMEM((width, 2 * ff), BF), pltpu.VMEM((ff, width), BF)
    (result,) = call(
        ffn_kernel, "ffn", [((slots, width), BF)], vm(1) + hb(6), 32,
        [into, into, outof, outof, pltpu.SemaphoreType.DMA((6,))],
    )(arrived.reshape(slots, width), wg, wu, wd, wg2, wu2, wd2)
    result, kv_all = lax.optimization_barrier((result, kv_all))
    returned = lax.all_to_all(result.reshape(experts, half, width), ep, 0, 0, tiled=True)
    near, far = ([(i, i ^ k) for i in range(xs)] for k in (1, 2))
    kv_near = lax.ppermute(kv_all, "x", near)
    own_part, far_part = call(attend_kernel, "attend", [((tok, 128), BF)] * 2, SM + vm(4), 24)(
        where, q_own, q_far, kv_all, kv_near
    )
    back = lax.ppermute(far_part, "x", far)
    keep_mix, send_mix = call(
        mix_kernel, "mix", [((ys, 8, width), BF)] * 2, SM + vm(3), 16, [pltpu.VMEM((tok, width), F32)]
    )(where, own_part, back, w_out)
    got_mix = lax.ppermute(send_mix, "c", swap)
    mix_half = (keep_mix.astype(F32) + got_mix.astype(F32)).astype(BF)
    mix_rows = mix_half.reshape(ys, 8, width // 128, 128).transpose(0, 2, 1, 3).reshape(ys, width // 16, 128)

    returned, mix_rows = lax.optimization_barrier((returned, mix_rows))
    keep, send = call(
        combine_kernel, "combine", [((ys, tok, 128), F32), ((ys, tok, 128), BF)], SM + vm(2), 16
    )(cs, returned.reshape(slots, width), spread)
    got = lax.ppermute(send, "c", swap)
    moe_half = (keep + got.astype(F32)).astype(BF)
    last = lax.all_to_all(jnp.concatenate([moe_half, mix_rows], axis=1), "y", 0, 0, tiled=True)
    summed = jnp.sum(last.astype(F32), axis=0).astype(BF)
    expert_out = summed[:tok]
    mixer_out = summed[tok:].reshape(width // 128, 8, 128).transpose(1, 0, 2).reshape(8, width)
    return mixer_out, expert_out


def solution(mesh):
    fine = Mesh(mesh.devices.reshape(8, 4, 8, 2), ("z", "x", "y", "c"))
    e, t = ("z", "x"), ("y", "c")
    in_specs = (
        P(e, t), P(e, None), P(e, None), P(), P(None, t), P(t, None), P(e, None), P(),
        P(e, None), P(e, None), P(e, None), P(e, None, t), P(e, None, t), P(e, t, None),
    )
    out_specs = (P(e + t, None), P(e, t))
    return jax.shard_map(per_device, mesh=fine, in_specs=in_specs, out_specs=out_specs, check_vma=False)
```

```python
import functools

import jax
import jax.numpy as jnp
from jax import lax
from jax.experimental import pallas as pl
from jax.experimental.pallas import tpu as pltpu
from jax.sharding import Mesh, PartitionSpec as P

PLAIN = 64
ROT = 32
VAL = 64
SEG = 64
GROUPS = 4
BF = jnp.bfloat16
F32 = jnp.float32
MIB = 1024 * 1024


def turn(v, cos, sin):
    a, b = v[: ROT // 2].astype(F32), v[ROT // 2 :].astype(F32)
    return jnp.concatenate([a * cos - b * sin, b * cos + a * sin], axis=0)


def fetch(pairs, sems):
    copies = [pltpu.make_async_copy(src, dst, sems.at[i]) for i, (src, dst) in enumerate(pairs)]
    for cp in copies:
        cp.start()
    return copies


def choose(c, pick_ref, experts):
    tok = pick_ref.shape[1]
    eid = lax.broadcasted_iota(jnp.int32, (experts, tok), 0)
    hit0, hit1 = eid == pick_ref[0:1, :], eid == pick_ref[1:2, :]
    hit = hit0 | hit1
    before = lax.broadcasted_iota(jnp.int32, (tok, tok), 0) < lax.broadcasted_iota(jnp.int32, (tok, tok), 1)
    rank = jnp.dot(
        jnp.where(hit, 1.0, 0.0).astype(BF), jnp.where(before, 1.0, 0.0).astype(BF), preferred_element_type=F32
    )
    code = jnp.where(hit, rank, -1.0)
    slot = (lax.broadcasted_iota(jnp.int32, (8, tok), 0) + 8 * c).astype(F32)
    sel = jnp.concatenate([jnp.where(code[e : e + 1, :] == slot, 1.0, 0.0) for e in range(experts)], axis=0)
    return hit0, hit1, sel


def keys_kernel(
    c_ref, lat_hbm, rot_hbm, cos_ref, sin_ref, gain_hbm, up_hbm, pick_hbm, gl_hbm, il_hbm,
    o_ref, w_ref, lat_ref, rot_ref, gain_ref, up_ref, pick_ref, gl_ref, il_ref, sems,
):
    pairs = (
        (lat_hbm, lat_ref), (gain_hbm, gain_ref), (up_hbm, up_ref), (rot_hbm, rot_ref),
        (pick_hbm, pick_ref), (gl_hbm, gl_ref), (il_hbm, il_ref),
    )
    for cp in fetch(pairs, sems):
        cp.wait()
    lat = lat_ref[...].astype(F32)
    lat = (lat * lax.rsqrt(jnp.mean(lat * lat, axis=1, keepdims=True) + 1e-06) * gain_ref[...]).astype(BF)
    kv = jnp.dot(lat, up_ref[...], preferred_element_type=F32).T
    rot = turn(rot_ref[...], cos_ref[...], sin_ref[...])
    pack = jnp.concatenate([kv[:PLAIN], rot, kv[PLAIN:]], axis=0).astype(BF)
    for b in range(o_ref.shape[0]):
        o_ref[b] = pack

    experts = w_ref.shape[1] // 16
    tok = w_ref.shape[0]
    hit0, hit1, sel = choose(c_ref[0], pick_ref, experts)
    gl = gl_ref[...]
    home = pick_ref[0:1, :] // (experts // GROUPS)
    gid = lax.broadcasted_iota(jnp.int32, (GROUPS, tok), 0)
    own = jnp.sum(jnp.where(gid == home, gl, 0.0), axis=0, keepdims=True)
    share = 1.0 / jnp.sum(jnp.exp(gl - own), axis=0, keepdims=True)
    gap = il_ref[0:1, :] - il_ref[1:2, :]
    first = share * (1.0 / (1.0 + jnp.exp(-gap)))
    second = share * (1.0 / (1.0 + jnp.exp(gap)))
    weight = jnp.where(hit0, first, 0.0) + jnp.where(hit1, second, 0.0)
    spread = sel * jnp.concatenate([jnp.broadcast_to(weight[e : e + 1, :], (8, tok)) for e in range(experts)], axis=0)
    hi = spread.astype(BF).astype(F32)
    w_ref[...] = jnp.concatenate([hi, spread - hi], axis=0).T.astype(BF)


def rows_kernel(c_ref, tok_hbm, gain_hbm, pick_hbm, o_ref, tok_ref, gain_ref, pick_ref, sems):
    cps = fetch(((pick_hbm, pick_ref), (tok_hbm, tok_ref), (gain_hbm, gain_ref)), sems)
    cps[0].wait()
    _, _, sel = choose(c_ref[0], pick_ref, o_ref.shape[0] // 8)
    cps[1].wait()
    cps[2].wait()
    vals = tok_ref[...].astype(F32)
    cen = vals - jnp.mean(vals, axis=1, keepdims=True)
    var = jnp.mean(cen * cen, axis=1, keepdims=True)
    normed = (cen * lax.rsqrt(var + 1e-05) * gain_ref[...]).astype(BF)
    o_ref[...] = jnp.dot(sel.astype(BF), normed, preferred_element_type=F32).astype(BF)


def split3(v):
    hi = v.astype(BF).astype(F32)
    rest = v - hi
    mid = rest.astype(BF).astype(F32)
    return hi, mid, rest - mid


def query_kernel(q_ref, cos_ref, sin_ref, o_ref):
    q = jnp.concatenate([q_ref[:PLAIN].astype(F32), turn(q_ref[PLAIN:], cos_ref[...], sin_ref[...])], axis=0)
    o_ref[...] = q.T.astype(BF)


def attend_kernel(where_ref, q0, q1, q2, q3, kv_ref, o0, o1, o2, o3):
    z, x = where_ref[0], where_ref[1]
    xs = 4
    zs, _, tok = kv_ref.shape
    segs = tok // SEG
    keys = jnp.concatenate([kv_ref[b, : PLAIN + ROT, :] for b in range(zs)], axis=1)
    vals = jnp.concatenate([kv_ref[b, PLAIN + ROT :, :] for b in range(zs)], axis=1)
    col = lax.broadcasted_iota(jnp.int32, (1, zs * tok), 1)
    key_seg = ((col // tok) * xs + x) * segs + (col % tok) // SEG
    row = lax.broadcasted_iota(jnp.int32, (tok, 1), 0)
    scale = (PLAIN + ROT) ** -0.5
    lane = lax.broadcasted_iota(jnp.int32, (tok, 128), 1)
    for k, (q_ref, o_ref) in enumerate(((q0, o0), (q1, o1), (q2, o2), (q3, o3))):
        xq = lax.rem(x + xs - k, xs)
        q_seg = (z * xs + xq) * segs + row // SEG
        s = jnp.dot(q_ref[...], keys, preferred_element_type=F32) * scale
        s = jnp.where(q_seg >= key_seg, s, -3e38)
        m = jnp.maximum(jnp.max(s, axis=1, keepdims=True), -1e30)
        p = jnp.exp(s - m)
        l = jnp.sum(p, axis=1, keepdims=True)
        acc = lax.dot_general(p.astype(BF), vals, (((1,), (1,)), ((), ())), preferred_element_type=F32)
        out = jnp.concatenate([acc, jnp.zeros((tok, 128 - VAL), F32)], axis=1)
        for i, piece in enumerate(split3(m) + split3(l)):
            out = jnp.where(lane == VAL + i, piece, out)
        o_ref[...] = out.astype(BF)


def mix_kernel(where_ref, a0, a1, a2, a3, w_ref, keep_ref, send_ref, res_ref):
    c = where_ref[2]
    parts = [r[...].astype(F32) for r in (a0, a1, a2, a3)]
    ms = [p[:, VAL : VAL + 1] + p[:, VAL + 1 : VAL + 2] + p[:, VAL + 2 : VAL + 3] for p in parts]
    ls = [p[:, VAL + 3 : VAL + 4] + p[:, VAL + 4 : VAL + 5] + p[:, VAL + 5 : VAL + 6] for p in parts]
    m = functools.reduce(jnp.maximum, ms)
    total = denom = 0.0
    for p, mp, lp in zip(parts, ms, ls):
        w = jnp.exp(mp - m)
        total = total + w * p[:, :VAL]
        denom = denom + w * lp
    attended = (total / denom).astype(BF)
    res_ref[...] = jnp.dot(attended, w_ref[...], preferred_element_type=F32)
    for y in range(keep_ref.shape[0]):
        keep_ref[y] = res_ref[pl.ds(pl.multiple_of(16 * y + 8 * c, 8), 8), :].astype(BF)
        send_ref[y] = res_ref[pl.ds(pl.multiple_of(16 * y + 8 * (1 - c), 8), 8), :].astype(BF)


def ffn_kernel(x_ref, g0h, u0h, d0h, g1h, u1h, d1h, o_ref, gu0, gu1, d0, d1, sems):
    f = d0.shape[0]
    cps = fetch((
        (g0h, gu0.at[:, :f]), (u0h, gu0.at[:, f:]), (g1h, gu1.at[:, :f]), (u1h, gu1.at[:, f:]), (d0h, d0), (d1h, d1)
    ), sems)
    rows = x_ref[...]
    hs = []
    for i, gu_ref in enumerate((gu0, gu1)):
        cps[2 * i].wait()
        cps[2 * i + 1].wait()
        both = jnp.dot(rows, gu_ref[...], preferred_element_type=F32)
        g, u = both[:, :f], both[:, f:]
        hs.append((g / (1.0 + jnp.exp(-g)) * u).astype(BF))
    cps[4].wait()
    cps[5].wait()
    acc = jnp.dot(hs[0], d0[...], preferred_element_type=F32) + jnp.dot(hs[1], d1[...], preferred_element_type=F32)
    o_ref[...] = acc.astype(BF)


def combine_kernel(c_ref, r_ref, w_ref, keep_ref, send_ref):
    c = c_ref[0]
    for i, o_ref in ((c, keep_ref), (1 - c, send_ref)):
        cols = jnp.concatenate(
            [r_ref[:, pl.ds(pl.multiple_of(128 * (2 * y + i), 128), 128)] for y in range(o_ref.shape[0])], axis=1
        )
        both = jnp.concatenate([cols, cols], axis=0)
        out = jnp.dot(w_ref[...], both, preferred_element_type=F32)
        for y in range(o_ref.shape[0]):
            o_ref[y] = out[:, 128 * y : 128 * (y + 1)].astype(o_ref.dtype)


def vm(n):
    return [pl.BlockSpec(memory_space=pltpu.VMEM)] * n


def hb(n):
    return [pl.BlockSpec(memory_space=pltpu.HBM)] * n


SM = [pl.BlockSpec(memory_space=pltpu.SMEM)]


def call(kernel, name, outs, ins, mib, scratch=()):
    return pl.pallas_call(
        kernel,
        out_shape=[jax.ShapeDtypeStruct(shape, dtype) for shape, dtype in outs],
        in_specs=ins,
        out_specs=vm(len(outs)),
        scratch_shapes=list(scratch),
        cost_estimate=pl.CostEstimate(flops=1000000, bytes_accessed=0, transcendentals=0),
        name=name,
        compiler_params=pltpu.CompilerParams(vmem_limit_bytes=mib * MIB),
    )


def per_device(
    queries, token_latents, key_rotary, latent_norm_gain, latent_up_weight, w_out,
    tokens_b, moe_gain, group_logits, inner_logits, expert_pick, w_gate, w_up, w_down,
):
    ep = ("z", "x")
    zs, xs, ys = lax.axis_size("z"), lax.axis_size("x"), lax.axis_size("y")
    z, x, c = (lax.axis_index(n).astype(jnp.int32) for n in ("z", "x", "c"))
    tok = queries.shape[0]
    width = tokens_b.shape[1]
    experts = zs * xs
    half = 8
    slots = experts * half
    ff = w_gate.shape[2]
    swap = [(0, 1), (1, 0)]

    positions = ((z * xs + x) * tok + jnp.arange(tok, dtype=jnp.int32)).astype(F32)
    freq = jnp.power(10000.0, -jnp.arange(ROT // 2, dtype=F32) * 2.0 / ROT)
    ang = freq[:, None] * positions[None, :]
    cos, sin = jnp.cos(ang), jnp.sin(ang)

    where = jnp.stack([z, x, c])
    cs = c.reshape(1)
    (outbound,) = call(
        rows_kernel, "rows", [((slots, width), BF)], SM + hb(3), 24,
        [
            pltpu.VMEM((tok, width), BF), pltpu.VMEM((1, width), F32), pltpu.VMEM((2, tok), jnp.int32),
            pltpu.SemaphoreType.DMA((3,)),
        ],
    )(cs, tokens_b, moe_gain[None, :], expert_pick.T)
    arrived = lax.all_to_all(outbound.reshape(experts, half, width), ep, 0, 0, tiled=True)

    wg, wu, wd = w_gate[0], w_up[0], w_down[0]
    wg2, wu2, wd2 = (lax.ppermute(w, "c", swap) for w in (wg, wu, wd))

    lat_w = token_latents.shape[1]
    pack, spread = call(
        keys_kernel, "keys", [((zs, PLAIN + ROT + VAL, tok), BF), ((tok, 2 * slots), BF)],
        SM + hb(2) + vm(2) + hb(5), 16,
        [
            pltpu.VMEM((tok, lat_w), BF), pltpu.VMEM((ROT, tok), BF), pltpu.VMEM((1, lat_w), F32),
            pltpu.VMEM((lat_w, PLAIN + VAL), BF), pltpu.VMEM((2, tok), jnp.int32),
            pltpu.VMEM((GROUPS, tok), F32), pltpu.VMEM((2, tok), F32), pltpu.SemaphoreType.DMA((7,)),
        ],
    )(
        cs, token_latents, key_rotary.T, cos, sin, latent_norm_gain[None, :], latent_up_weight,
        expert_pick.T, group_logits.T, inner_logits.T,
    )
    (q_own,) = call(query_kernel, "query", [((tok, PLAIN + ROT), BF)], vm(3), 16)(queries.T, cos, sin)
    qs = [q_own] + [
        lax.ppermute(q_own, "x", [(i, (i + k) % xs) for i in range(xs)]) for k in range(1, xs)
    ]
    arrived, pack, qs = lax.optimization_barrier((arrived, pack, qs))
    kv_all = lax.all_to_all(pack, "z", 0, 0, tiled=True)
    into, outof = pltpu.VMEM((width, 2 * ff), BF), pltpu.VMEM((ff, width), BF)
    (result,) = call(
        ffn_kernel, "ffn", [((slots, width), BF)], vm(1) + hb(6), 32,
        [into, into, outof, outof, pltpu.SemaphoreType.DMA((6,))],
    )(arrived.reshape(slots, width), wg, wu, wd, wg2, wu2, wd2)
    result, kv_all = lax.optimization_barrier((result, kv_all))
    returned = lax.all_to_all(result.reshape(experts, half, width), ep, 0, 0, tiled=True)
    parts = call(attend_kernel, "attend", [((tok, 128), BF)] * xs, SM + vm(5), 16)(where, *qs, kv_all)
    back = [parts[0]] + [
        lax.ppermute(parts[k], "x", [(i, (i - k) % xs) for i in range(xs)]) for k in range(1, xs)
    ]
    keep_mix, send_mix = call(
        mix_kernel, "mix", [((ys, 8, width), BF)] * 2, SM + vm(5), 16, [pltpu.VMEM((tok, width), F32)]
    )(where, *back, w_out)
    got_mix = lax.ppermute(send_mix, "c", swap)
    mix_half = (keep_mix.astype(F32) + got_mix.astype(F32)).astype(BF)
    mix_rows = mix_half.reshape(ys, 8, width // 128, 128).transpose(0, 2, 1, 3).reshape(ys, width // 16, 128)

    returned, mix_rows = lax.optimization_barrier((returned, mix_rows))
    keep, send = call(
        combine_kernel, "combine", [((ys, tok, 128), F32), ((ys, tok, 128), BF)], SM + vm(2), 16
    )(cs, returned.reshape(slots, width), spread)
    got = lax.ppermute(send, "c", swap)
    moe_half = (keep + got.astype(F32)).astype(BF)
    last = lax.all_to_all(jnp.concatenate([moe_half, mix_rows], axis=1), "y", 0, 0, tiled=True)
    summed = jnp.sum(last.astype(F32), axis=0).astype(BF)
    expert_out = summed[:tok]
    mixer_out = summed[tok:].reshape(width // 128, 8, 128).transpose(1, 0, 2).reshape(8, width)
    return mixer_out, expert_out


def solution(mesh):
    fine = Mesh(mesh.devices.reshape(8, 4, 8, 2), ("z", "x", "y", "c"))
    e, t = ("z", "x"), ("y", "c")
    in_specs = (
        P(e, t), P(e, None), P(e, None), P(), P(None, t), P(t, None), P(e, None), P(),
        P(e, None), P(e, None), P(e, None), P(e, None, t), P(e, None, t), P(e, t, None),
    )
    out_specs = (P(e + t, None), P(e, t))
    return jax.shard_map(per_device, mesh=fine, in_specs=in_specs, out_specs=out_specs, check_vma=False)
```

```python
import functools

import jax
import jax.numpy as jnp
from jax import lax
from jax.experimental import pallas as pl
from jax.experimental.pallas import tpu as pltpu
from jax.sharding import Mesh, PartitionSpec as P

PLAIN = 64
ROT = 32
VAL = 64
SEG = 64
GROUPS = 4
BF = jnp.bfloat16
F32 = jnp.float32
MIB = 1024 * 1024


def turn(v, cos, sin):
    a, b = v[: ROT // 2].astype(F32), v[ROT // 2 :].astype(F32)
    return jnp.concatenate([a * cos - b * sin, b * cos + a * sin], axis=0)


def fetch(pairs, sems):
    copies = [pltpu.make_async_copy(src, dst, sems.at[i]) for i, (src, dst) in enumerate(pairs)]
    for cp in copies:
        cp.start()
    return copies


def choose(pick_ref, experts, base, count):
    tok = pick_ref.shape[1]
    eid = lax.broadcasted_iota(jnp.int32, (experts, tok), 0)
    hit0, hit1 = eid == pick_ref[0:1, :], eid == pick_ref[1:2, :]
    hit = hit0 | hit1
    before = lax.broadcasted_iota(jnp.int32, (tok, tok), 0) < lax.broadcasted_iota(jnp.int32, (tok, tok), 1)
    rank = jnp.dot(
        jnp.where(hit, 1.0, 0.0).astype(BF), jnp.where(before, 1.0, 0.0).astype(BF), preferred_element_type=F32
    )
    code = jnp.where(hit, rank, -1.0)
    slot = (lax.broadcasted_iota(jnp.int32, (count, tok), 0) + base).astype(F32)
    sel = jnp.concatenate([jnp.where(code[e : e + 1, :] == slot, 1.0, 0.0) for e in range(experts)], axis=0)
    return hit0, hit1, sel


def keys_kernel(
    lat_hbm, rot_hbm, cos_ref, sin_ref, gain_hbm, up_hbm, pick_hbm, gl_hbm, il_hbm,
    o_ref, w_ref, lat_ref, rot_ref, gain_ref, up_ref, pick_ref, gl_ref, il_ref, sems,
):
    pairs = (
        (lat_hbm, lat_ref), (gain_hbm, gain_ref), (up_hbm, up_ref), (rot_hbm, rot_ref),
        (pick_hbm, pick_ref), (gl_hbm, gl_ref), (il_hbm, il_ref),
    )
    for cp in fetch(pairs, sems):
        cp.wait()
    lat = lat_ref[...].astype(F32)
    lat = (lat * lax.rsqrt(jnp.mean(lat * lat, axis=1, keepdims=True) + 1e-06) * gain_ref[...]).astype(BF)
    kv = jnp.dot(lat, up_ref[...], preferred_element_type=F32).T
    rot = turn(rot_ref[...], cos_ref[...], sin_ref[...])
    pack = jnp.concatenate([kv[:PLAIN], rot, kv[PLAIN:]], axis=0).astype(BF)
    for b in range(o_ref.shape[0]):
        o_ref[b] = pack

    experts = w_ref.shape[1] // 32
    tok = w_ref.shape[0]
    hit0, hit1, sel = choose(pick_ref, experts, 0, 16)
    gl = gl_ref[...]
    home = pick_ref[0:1, :] // (experts // GROUPS)
    gid = lax.broadcasted_iota(jnp.int32, (GROUPS, tok), 0)
    own = jnp.sum(jnp.where(gid == home, gl, 0.0), axis=0, keepdims=True)
    share = 1.0 / jnp.sum(jnp.exp(gl - own), axis=0, keepdims=True)
    gap = il_ref[0:1, :] - il_ref[1:2, :]
    first = share * (1.0 / (1.0 + jnp.exp(-gap)))
    second = share * (1.0 / (1.0 + jnp.exp(gap)))
    weight = jnp.where(hit0, first, 0.0) + jnp.where(hit1, second, 0.0)
    spread = sel * jnp.concatenate([jnp.broadcast_to(weight[e : e + 1, :], (16, tok)) for e in range(experts)], axis=0)
    hi = spread.astype(BF).astype(F32)
    w_ref[...] = jnp.concatenate([hi, spread - hi], axis=0).T.astype(BF)


def rows_kernel(c_ref, tok_hbm, gain_hbm, pick_hbm, o_ref, tok_ref, gain_ref, pick_ref, sems):
    cps = fetch(((pick_hbm, pick_ref), (tok_hbm, tok_ref), (gain_hbm, gain_ref)), sems)
    cps[0].wait()
    _, _, sel = choose(pick_ref, o_ref.shape[0] // 8, 8 * c_ref[0], 8)
    cps[1].wait()
    cps[2].wait()
    vals = tok_ref[...].astype(F32)
    cen = vals - jnp.mean(vals, axis=1, keepdims=True)
    var = jnp.mean(cen * cen, axis=1, keepdims=True)
    normed = (cen * lax.rsqrt(var + 1e-05) * gain_ref[...]).astype(BF)
    o_ref[...] = jnp.dot(sel.astype(BF), normed, preferred_element_type=F32).astype(BF)


def split3(v):
    hi = v.astype(BF).astype(F32)
    rest = v - hi
    mid = rest.astype(BF).astype(F32)
    return hi, mid, rest - mid


def query_kernel(q_ref, cos_ref, sin_ref, o_ref):
    q = jnp.concatenate([q_ref[:PLAIN].astype(F32), turn(q_ref[PLAIN:], cos_ref[...], sin_ref[...])], axis=0)
    o_ref[...] = q.T.astype(BF)


def attend_kernel(where_ref, q0, q1, q2, q3, kv_ref, o0, o1, o2, o3):
    z, x = where_ref[0], where_ref[1]
    xs = 4
    zs, _, tok = kv_ref.shape
    segs = tok // SEG
    keys = jnp.concatenate([kv_ref[b, : PLAIN + ROT, :] for b in range(zs)], axis=1)
    vals = jnp.concatenate([kv_ref[b, PLAIN + ROT :, :] for b in range(zs)], axis=1)
    col = lax.broadcasted_iota(jnp.int32, (1, zs * tok), 1)
    key_seg = ((col // tok) * xs + x) * segs + (col % tok) // SEG
    row = lax.broadcasted_iota(jnp.int32, (tok, 1), 0)
    scale = (PLAIN + ROT) ** -0.5
    lane = lax.broadcasted_iota(jnp.int32, (tok, 128), 1)
    for k, (q_ref, o_ref) in enumerate(((q0, o0), (q1, o1), (q2, o2), (q3, o3))):
        xq = lax.rem(x + xs - k, xs)
        q_seg = (z * xs + xq) * segs + row // SEG
        s = jnp.dot(q_ref[...], keys, preferred_element_type=F32) * scale
        s = jnp.where(q_seg >= key_seg, s, -3e38)
        m = jnp.maximum(jnp.max(s, axis=1, keepdims=True), -1e30)
        p = jnp.exp(s - m)
        l = jnp.sum(p, axis=1, keepdims=True)
        acc = lax.dot_general(p.astype(BF), vals, (((1,), (1,)), ((), ())), preferred_element_type=F32)
        out = jnp.concatenate([acc, jnp.zeros((tok, 128 - VAL), F32)], axis=1)
        for i, piece in enumerate(split3(m) + split3(l)):
            out = jnp.where(lane == VAL + i, piece, out)
        o_ref[...] = out.astype(BF)


def mix_kernel(where_ref, a0, a1, a2, a3, w_ref, keep_ref, send_ref, res_ref):
    c = where_ref[2]
    parts = [r[...].astype(F32) for r in (a0, a1, a2, a3)]
    ms = [p[:, VAL : VAL + 1] + p[:, VAL + 1 : VAL + 2] + p[:, VAL + 2 : VAL + 3] for p in parts]
    ls = [p[:, VAL + 3 : VAL + 4] + p[:, VAL + 4 : VAL + 5] + p[:, VAL + 5 : VAL + 6] for p in parts]
    m = functools.reduce(jnp.maximum, ms)
    total = denom = 0.0
    for p, mp, lp in zip(parts, ms, ls):
        w = jnp.exp(mp - m)
        total = total + w * p[:, :VAL]
        denom = denom + w * lp
    attended = (total / denom).astype(BF)
    res_ref[...] = jnp.dot(attended, w_ref[...], preferred_element_type=F32)
    for y in range(keep_ref.shape[0]):
        keep_ref[y] = res_ref[pl.ds(pl.multiple_of(16 * y + 8 * c, 8), 8), :].astype(BF)
        send_ref[y] = res_ref[pl.ds(pl.multiple_of(16 * y + 8 * (1 - c), 8), 8), :].astype(BF)


def hidden_kernel(x_ref, g0h, u0h, g1h, u1h, o_ref, gu0, gu1, sems):
    f = o_ref.shape[1] // 2
    cps = fetch(((g0h, gu0.at[:, :f]), (u0h, gu0.at[:, f:]), (g1h, gu1.at[:, :f]), (u1h, gu1.at[:, f:])), sems)
    rows = x_ref[...]
    for i, gu_ref in enumerate((gu0, gu1)):
        cps[2 * i].wait()
        cps[2 * i + 1].wait()
        both = jnp.dot(rows, gu_ref[...], preferred_element_type=F32)
        g, u = both[:, :f], both[:, f:]
        o_ref[:, i * f : (i + 1) * f] = (g / (1.0 + jnp.exp(-g)) * u).astype(BF)


def down_kernel(c_ref, h_ref, h2_ref, dh, d2h, o_ref, d, d2, sems):
    c = c_ref[0]
    f = d.shape[0]
    n = d.shape[1] // 128
    pairs = []
    for y in range(n):
        cols = pl.ds(pl.multiple_of(128 * (2 * y + c), 128), 128)
        pairs += [(dh.at[:, cols], d.at[:, 128 * y : 128 * y + 128]), (d2h.at[:, cols], d2.at[:, 128 * y : 128 * y + 128])]
    for cp in fetch(pairs, sems):
        cp.wait()
    for i, h, first, second in ((c, h_ref, d, d2), (1 - c, h2_ref, d2, d)):
        acc = jnp.dot(h[:, :f], first[...], preferred_element_type=F32) + jnp.dot(
            h[:, f:], second[...], preferred_element_type=F32
        )
        o_ref[:, pl.ds(i, 1)] = acc.astype(BF).reshape(o_ref.shape[0], 1, o_ref.shape[2], o_ref.shape[3])


def combine_kernel(r_ref, w_ref, mix_ref, o_ref):
    tok = w_ref.shape[0]
    both = jnp.concatenate([r_ref[...], r_ref[...]], axis=0)
    out = jnp.dot(w_ref[...], both, preferred_element_type=F32)
    for y in range(o_ref.shape[0]):
        o_ref[y, :tok] = out[:, 128 * y : 128 * (y + 1)].astype(BF)
        o_ref[y, tok:] = mix_ref[y]


def vm(n):
    return [pl.BlockSpec(memory_space=pltpu.VMEM)] * n


def hb(n):
    return [pl.BlockSpec(memory_space=pltpu.HBM)] * n


SM = [pl.BlockSpec(memory_space=pltpu.SMEM)]


def call(kernel, name, outs, ins, mib, scratch=()):
    return pl.pallas_call(
        kernel,
        out_shape=[jax.ShapeDtypeStruct(shape, dtype) for shape, dtype in outs],
        in_specs=ins,
        out_specs=vm(len(outs)),
        scratch_shapes=list(scratch),
        cost_estimate=pl.CostEstimate(flops=1000000, bytes_accessed=0, transcendentals=0),
        name=name,
        compiler_params=pltpu.CompilerParams(vmem_limit_bytes=int(mib * MIB)),
    )


def per_device(
    queries, token_latents, key_rotary, latent_norm_gain, latent_up_weight, w_out,
    tokens_b, moe_gain, group_logits, inner_logits, expert_pick, w_gate, w_up, w_down,
):
    ep = ("z", "x")
    zs, xs, ys = lax.axis_size("z"), lax.axis_size("x"), lax.axis_size("y")
    z, x, c = (lax.axis_index(n).astype(jnp.int32) for n in ("z", "x", "c"))
    tok = queries.shape[0]
    width = tokens_b.shape[1]
    experts = zs * xs
    half = 8
    slots = experts * half
    ff = w_gate.shape[2]
    swap = [(0, 1), (1, 0)]

    positions = ((z * xs + x) * tok + jnp.arange(tok, dtype=jnp.int32)).astype(F32)
    freq = jnp.power(10000.0, -jnp.arange(ROT // 2, dtype=F32) * 2.0 / ROT)
    ang = freq[:, None] * positions[None, :]
    cos, sin = jnp.cos(ang), jnp.sin(ang)

    where = jnp.stack([z, x, c])
    cs = c.reshape(1)
    (outbound,) = call(
        rows_kernel, "rows", [((slots, width), BF)], SM + hb(3), 63.9,
        [
            pltpu.VMEM((tok, width), BF), pltpu.VMEM((1, width), F32), pltpu.VMEM((2, tok), jnp.int32),
            pltpu.SemaphoreType.DMA((3,)),
        ],
    )(cs, tokens_b, moe_gain[None, :], expert_pick.T)
    arrived = lax.all_to_all(outbound.reshape(experts, half, width), ep, 0, 0, tiled=True)

    wg, wu, wd = w_gate[0], w_up[0], w_down[0]
    wg2, wu2, wd2 = (lax.ppermute(w, "c", swap) for w in (wg, wu, wd))

    lat_w = token_latents.shape[1]
    pack, spread = call(
        keys_kernel, "keys", [((zs, PLAIN + ROT + VAL, tok), BF), ((tok, 4 * slots), BF)],
        hb(2) + vm(2) + hb(5), 16,
        [
            pltpu.VMEM((tok, lat_w), BF), pltpu.VMEM((ROT, tok), BF), pltpu.VMEM((1, lat_w), F32),
            pltpu.VMEM((lat_w, PLAIN + VAL), BF), pltpu.VMEM((2, tok), jnp.int32),
            pltpu.VMEM((GROUPS, tok), F32), pltpu.VMEM((2, tok), F32), pltpu.SemaphoreType.DMA((7,)),
        ],
    )(
        token_latents, key_rotary.T, cos, sin, latent_norm_gain[None, :], latent_up_weight,
        expert_pick.T, group_logits.T, inner_logits.T,
    )
    (q_own,) = call(query_kernel, "query", [((tok, PLAIN + ROT), BF)], vm(3), 16)(queries.T, cos, sin)
    qs = [q_own] + [
        lax.ppermute(q_own, "x", [(i, (i + k) % xs) for i in range(xs)]) for k in range(1, xs)
    ]
    arrived, pack, qs = lax.optimization_barrier((arrived, pack, qs))
    kv_all = lax.all_to_all(pack, "z", 0, 0, tiled=True)
    into, outof = pltpu.VMEM((width, 2 * ff), BF), pltpu.VMEM((ff, width // 2), BF)
    (hid,) = call(
        hidden_kernel, "hidden", [((slots, 2 * ff), BF)], vm(1) + hb(4), 32,
        [into, into, pltpu.SemaphoreType.DMA((4,))],
    )(arrived.reshape(slots, width), wg, wu, wg2, wu2)
    hid2 = lax.ppermute(hid, "c", swap)
    (result,) = call(
        down_kernel, "down", [((experts, 2, half, width // 2), BF)], SM + vm(2) + hb(2), 32,
        [outof, outof, pltpu.SemaphoreType.DMA((2 * ys,))],
    )(cs, hid, hid2, wd, wd2)
    result, kv_all = lax.optimization_barrier((result, kv_all))
    returned = lax.all_to_all(result.reshape(experts, 2 * half, width // 2), ep, 0, 0, tiled=True)
    parts = call(attend_kernel, "attend", [((tok, 128), BF)] * xs, SM + vm(5), 16)(where, *qs, kv_all)
    back = [parts[0]] + [
        lax.ppermute(parts[k], "x", [(i, (i - k) % xs) for i in range(xs)]) for k in range(1, xs)
    ]
    keep_mix, send_mix = call(
        mix_kernel, "mix", [((ys, 8, width), BF)] * 2, SM + vm(5), 16, [pltpu.VMEM((tok, width), F32)]
    )(where, *back, w_out)
    got_mix = lax.ppermute(send_mix, "c", swap)
    mix_half = (keep_mix.astype(F32) + got_mix.astype(F32)).astype(BF)
    mix_rows = mix_half.reshape(ys, 8, width // 128, 128).transpose(0, 2, 1, 3).reshape(ys, width // 16, 128)

    returned, mix_rows = lax.optimization_barrier((returned, mix_rows))
    (partial_sums,) = call(combine_kernel, "combine", [((ys, 2 * tok, 128), BF)], vm(3), 16)(
        returned.reshape(2 * slots, width // 2), spread, mix_rows
    )
    last = lax.all_to_all(partial_sums, "y", 0, 0, tiled=True)
    summed = jnp.sum(last.astype(F32), axis=0).astype(BF)
    expert_out = summed[:tok]
    mixer_out = summed[tok:].reshape(width // 128, 8, 128).transpose(1, 0, 2).reshape(8, width)
    return mixer_out, expert_out


def solution(mesh):
    fine = Mesh(mesh.devices.reshape(8, 4, 8, 2), ("z", "x", "y", "c"))
    e, t = ("z", "x"), ("y", "c")
    in_specs = (
        P(e, t), P(e, None), P(e, None), P(), P(None, t), P(t, None), P(e, None), P(),
        P(e, None), P(e, None), P(e, None), P(e, None, t), P(e, None, t), P(e, t, None),
    )
    out_specs = (P(e + t, None), P(e, t))
    return jax.shard_map(per_device, mesh=fine, in_specs=in_specs, out_specs=out_specs, check_vma=False)
```

```python
import functools

import jax
import jax.numpy as jnp
from jax import lax
from jax.experimental import pallas as pl
from jax.experimental.pallas import tpu as pltpu
from jax.sharding import Mesh, PartitionSpec as P

PLAIN = 64
ROT = 32
VAL = 64
SEG = 64
GROUPS = 4
BF = jnp.bfloat16
F32 = jnp.float32
MIB = 1024 * 1024


def turn(v, cos, sin):
    a, b = v[: ROT // 2].astype(F32), v[ROT // 2 :].astype(F32)
    return jnp.concatenate([a * cos - b * sin, b * cos + a * sin], axis=0)


def fetch(pairs, sems):
    copies = [pltpu.make_async_copy(src, dst, sems.at[i]) for i, (src, dst) in enumerate(pairs)]
    for cp in copies:
        cp.start()
    return copies


def choose(pick_ref, experts, base, count):
    tok = pick_ref.shape[1]
    eid = lax.broadcasted_iota(jnp.int32, (experts, tok), 0)
    hit0, hit1 = eid == pick_ref[0:1, :], eid == pick_ref[1:2, :]
    hit = hit0 | hit1
    before = lax.broadcasted_iota(jnp.int32, (tok, tok), 0) < lax.broadcasted_iota(jnp.int32, (tok, tok), 1)
    rank = jnp.dot(
        jnp.where(hit, 1.0, 0.0).astype(BF), jnp.where(before, 1.0, 0.0).astype(BF), preferred_element_type=F32
    )
    code = jnp.where(hit, rank, -1.0)
    slot = (lax.broadcasted_iota(jnp.int32, (count, tok), 0) + base).astype(F32)
    sel = jnp.concatenate([jnp.where(code[e : e + 1, :] == slot, 1.0, 0.0) for e in range(experts)], axis=0)
    return hit0, hit1, sel


def rows_kernel(
    c_ref, cos_ref, sin_ref, tok_hbm, gain_hbm, pick_hbm, lat_hbm, lgain_hbm, up_hbm, rot_hbm,
    o_ref, tok_ref, gain_ref, pick_ref, lat_ref, lgain_ref, up_ref, rot_ref, sems,
):
    cps = fetch((
        (lat_hbm, lat_ref), (lgain_hbm, lgain_ref), (up_hbm, up_ref), (rot_hbm, rot_ref),
        (pick_hbm, pick_ref), (tok_hbm, tok_ref), (gain_hbm, gain_ref),
    ), sems)
    width = tok_ref.shape[1]
    experts = o_ref.shape[0] // 8
    for cp in cps[:4]:
        cp.wait()
    lat = lat_ref[...].astype(F32)
    lat = (lat * lax.rsqrt(jnp.mean(lat * lat, axis=1, keepdims=True) + 1e-06) * lgain_ref[...]).astype(BF)
    kv = jnp.dot(lat, up_ref[...], preferred_element_type=F32)
    rot = turn(rot_ref[...], cos_ref[...], sin_ref[...]).T
    blocks = []
    for q in range(4):
        rows = [slice(32 * q + 8 * i, 32 * q + 8 * i + 8) for i in range(4)]
        blocks.append(jnp.concatenate([kv[r] for r in rows] + [rot[r] for r in rows], axis=1).astype(BF))
    for e in range(experts):
        o_ref[8 * e : 8 * e + 8, width:] = blocks[e % 4]
    cps[4].wait()
    _, _, sel = choose(pick_ref, experts, 8 * c_ref[0], 8)
    cps[5].wait()
    cps[6].wait()
    vals = tok_ref[...].astype(F32)
    cen = vals - jnp.mean(vals, axis=1, keepdims=True)
    var = jnp.mean(cen * cen, axis=1, keepdims=True)
    normed = (cen * lax.rsqrt(var + 1e-05) * gain_ref[...]).astype(BF)
    o_ref[:, :width] = jnp.dot(sel.astype(BF), normed, preferred_element_type=F32).astype(BF)


def side_kernel(
    cos_ref, sin_ref, q_hbm, pick_hbm, gl_hbm, il_hbm, q_out, w_ref, q_ref, pick_ref, gl_ref, il_ref, sems
):
    for cp in fetch(((q_hbm, q_ref), (pick_hbm, pick_ref), (gl_hbm, gl_ref), (il_hbm, il_ref)), sems):
        cp.wait()
    q = jnp.concatenate([q_ref[:PLAIN].astype(F32), turn(q_ref[PLAIN:], cos_ref[...], sin_ref[...])], axis=0)
    q_out[...] = q.T.astype(BF)
    experts = w_ref.shape[1] // 32
    tok = w_ref.shape[0]
    hit0, hit1, sel = choose(pick_ref, experts, 0, 16)
    gl = gl_ref[...]
    home = pick_ref[0:1, :] // (experts // GROUPS)
    gid = lax.broadcasted_iota(jnp.int32, (GROUPS, tok), 0)
    own = jnp.sum(jnp.where(gid == home, gl, 0.0), axis=0, keepdims=True)
    share = 1.0 / jnp.sum(jnp.exp(gl - own), axis=0, keepdims=True)
    gap = il_ref[0:1, :] - il_ref[1:2, :]
    first = share * (1.0 / (1.0 + jnp.exp(-gap)))
    second = share * (1.0 / (1.0 + jnp.exp(gap)))
    weight = jnp.where(hit0, first, 0.0) + jnp.where(hit1, second, 0.0)
    spread = sel * jnp.concatenate([jnp.broadcast_to(weight[e : e + 1, :], (16, tok)) for e in range(experts)], axis=0)
    hi = spread.astype(BF).astype(F32)
    w_ref[...] = jnp.concatenate([hi, spread - hi], axis=0).T.astype(BF)


def split3(v):
    hi = v.astype(BF).astype(F32)
    rest = v - hi
    mid = rest.astype(BF).astype(F32)
    return hi, mid, rest - mid


def attend_kernel(where_ref, q0, q1, q2, q3, kv_ref, o0, o1, o2, o3):
    z, x = where_ref[0], where_ref[1]
    xs = 4
    tok = q0.shape[0]
    segs = tok // SEG
    count = kv_ref.shape[0]
    base = 4 * (PLAIN + VAL)
    keys = jnp.concatenate([
        jnp.concatenate([kv_ref[:, 128 * i : 128 * i + PLAIN], kv_ref[:, base + ROT * i : base + ROT * i + ROT]], axis=1)
        for i in range(4)
    ], axis=0)
    vals = jnp.concatenate([kv_ref[:, 128 * i + PLAIN : 128 * i + 128] for i in range(4)], axis=0)
    col = lax.broadcasted_iota(jnp.int32, (1, 4 * count), 1)
    part = (tok // xs) * x + 8 * (col // count) + col % 8
    key_seg = ((col % count) // 8) * segs + part // SEG
    row = lax.broadcasted_iota(jnp.int32, (tok, 1), 0)
    scale = (PLAIN + ROT) ** -0.5
    lane = lax.broadcasted_iota(jnp.int32, (tok, 128), 1)
    for k, (q_ref, o_ref) in enumerate(((q0, o0), (q1, o1), (q2, o2), (q3, o3))):
        xq = lax.rem(x + xs - k, xs)
        q_seg = (z * xs + xq) * segs + row // SEG
        s = lax.dot_general(q_ref[...], keys, (((1,), (1,)), ((), ())), preferred_element_type=F32) * scale
        s = jnp.where(q_seg >= key_seg, s, -3e38)
        m = jnp.maximum(jnp.max(s, axis=1, keepdims=True), -1e30)
        p = jnp.exp(s - m)
        l = jnp.sum(p, axis=1, keepdims=True)
        acc = jnp.dot(p.astype(BF), vals, preferred_element_type=F32)
        out = jnp.concatenate([acc, jnp.zeros((tok, 128 - VAL), F32)], axis=1)
        for i, piece in enumerate(split3(m) + split3(l)):
            out = jnp.where(lane == VAL + i, piece, out)
        o_ref[...] = out.astype(BF)


def mix_kernel(where_ref, a0, a1, a2, a3, w_ref, keep_ref, send_ref, res_ref):
    c = where_ref[2]
    parts = [r[...].astype(F32) for r in (a0, a1, a2, a3)]
    ms = [p[:, VAL : VAL + 1] + p[:, VAL + 1 : VAL + 2] + p[:, VAL + 2 : VAL + 3] for p in parts]
    ls = [p[:, VAL + 3 : VAL + 4] + p[:, VAL + 4 : VAL + 5] + p[:, VAL + 5 : VAL + 6] for p in parts]
    m = functools.reduce(jnp.maximum, ms)
    total = denom = 0.0
    for p, mp, lp in zip(parts, ms, ls):
        w = jnp.exp(mp - m)
        total = total + w * p[:, :VAL]
        denom = denom + w * lp
    attended = (total / denom).astype(BF)
    res_ref[...] = jnp.dot(attended, w_ref[...], preferred_element_type=F32)
    for y in range(keep_ref.shape[0]):
        keep_ref[y] = res_ref[pl.ds(pl.multiple_of(16 * y + 8 * c, 8), 8), :].astype(BF)
        send_ref[y] = res_ref[pl.ds(pl.multiple_of(16 * y + 8 * (1 - c), 8), 8), :].astype(BF)


def hidden_kernel(c_ref, xh, g0h, u0h, g1h, u1h, dh, d2h, o_ref, kv_ref, d, d2, x_ref, gu0, gu1, sems):
    c = c_ref[0]
    f = o_ref.shape[1] // 2
    pairs = [(xh, x_ref), (g0h, gu0.at[:, :f]), (u0h, gu0.at[:, f:]), (g1h, gu1.at[:, :f]), (u1h, gu1.at[:, f:])]
    for y in range(d.shape[1] // 128):
        cols = pl.ds(pl.multiple_of(128 * (2 * y + c), 128), 128)
        pairs += [(dh.at[:, cols], d.at[:, 128 * y : 128 * y + 128]), (d2h.at[:, cols], d2.at[:, 128 * y : 128 * y + 128])]
    cps = fetch(pairs, sems)
    cps[0].wait()
    kv_ref[...] = x_ref[:, gu0.shape[0] :]
    rows = x_ref[:, : gu0.shape[0]]
    for i, gu_ref in enumerate((gu0, gu1)):
        cps[2 * i + 1].wait()
        cps[2 * i + 2].wait()
        both = jnp.dot(rows, gu_ref[...], preferred_element_type=F32)
        g, u = both[:, :f], both[:, f:]
        o_ref[:, i * f : (i + 1) * f] = (g / (1.0 + jnp.exp(-g)) * u).astype(BF)
    for cp in cps[5:]:
        cp.wait()


def down_kernel(c_ref, h_ref, h2_ref, d, d2, o_ref):
    c = c_ref[0]
    f = d.shape[0]
    for i, h, first, second in ((c, h_ref, d, d2), (1 - c, h2_ref, d2, d)):
        acc = jnp.dot(h[:, :f], first[...], preferred_element_type=F32) + jnp.dot(
            h[:, f:], second[...], preferred_element_type=F32
        )
        o_ref[:, pl.ds(i, 1)] = acc.astype(BF).reshape(o_ref.shape[0], 1, o_ref.shape[2], o_ref.shape[3])


def combine_kernel(r_ref, w_ref, mix_ref, o_ref):
    tok = w_ref.shape[0]
    both = jnp.concatenate([r_ref[...], r_ref[...]], axis=0)
    out = jnp.dot(w_ref[...], both, preferred_element_type=F32)
    for y in range(o_ref.shape[0]):
        o_ref[y, :tok] = out[:, 128 * y : 128 * (y + 1)].astype(BF)
        o_ref[y, tok:] = mix_ref[y]


def vm(n):
    return [pl.BlockSpec(memory_space=pltpu.VMEM)] * n


def hb(n):
    return [pl.BlockSpec(memory_space=pltpu.HBM)] * n


SM = [pl.BlockSpec(memory_space=pltpu.SMEM)]


def call(kernel, name, outs, ins, mib, scratch=()):
    return pl.pallas_call(
        kernel,
        out_shape=[jax.ShapeDtypeStruct(shape, dtype) for shape, dtype in outs],
        in_specs=ins,
        out_specs=vm(len(outs)),
        scratch_shapes=list(scratch),
        cost_estimate=pl.CostEstimate(flops=1000000, bytes_accessed=0, transcendentals=0),
        name=name,
        compiler_params=pltpu.CompilerParams(vmem_limit_bytes=int(mib * MIB)),
    )


def per_device(
    queries, token_latents, key_rotary, latent_norm_gain, latent_up_weight, w_out,
    tokens_b, moe_gain, group_logits, inner_logits, expert_pick, w_gate, w_up, w_down,
):
    ep = ("z", "x")
    zs, xs, ys = lax.axis_size("z"), lax.axis_size("x"), lax.axis_size("y")
    z, x, c = (lax.axis_index(n).astype(jnp.int32) for n in ("z", "x", "c"))
    tok = queries.shape[0]
    width = tokens_b.shape[1]
    experts = zs * xs
    half = 8
    slots = experts * half
    ff = w_gate.shape[2]
    swap = [(0, 1), (1, 0)]

    positions = ((z * xs + x) * tok + jnp.arange(tok, dtype=jnp.int32)).astype(F32)
    freq = jnp.power(10000.0, -jnp.arange(ROT // 2, dtype=F32) * 2.0 / ROT)
    ang = freq[:, None] * positions[None, :]
    cos, sin = jnp.cos(ang), jnp.sin(ang)

    where = jnp.stack([z, x, c])
    cs = c.reshape(1)
    lat_w = token_latents.shape[1]
    kv_w = (tok // xs // 8) * (PLAIN + ROT + VAL)
    (outbound,) = call(
        rows_kernel, "rows", [((slots, width + kv_w), BF)], SM + vm(2) + hb(7), 63.9,
        [
            pltpu.VMEM((tok, width), BF), pltpu.VMEM((1, width), F32), pltpu.VMEM((2, tok), jnp.int32),
            pltpu.VMEM((tok, lat_w), BF), pltpu.VMEM((1, lat_w), F32), pltpu.VMEM((lat_w, PLAIN + VAL), BF),
            pltpu.VMEM((ROT, tok), BF), pltpu.SemaphoreType.DMA((7,)),
        ],
    )(
        cs, cos, sin, tokens_b, moe_gain[None, :], expert_pick.T, token_latents, latent_norm_gain[None, :],
        latent_up_weight, key_rotary.T,
    )
    arrived = lax.all_to_all(outbound.reshape(experts, half, width + kv_w), ep, 0, 0, tiled=True)

    wg, wu, wd = w_gate[0], w_up[0], w_down[0]
    wg2, wu2, wd2 = (lax.ppermute(w, "c", swap) for w in (wg, wu, wd))

    q_own, spread = call(
        side_kernel, "side", [((tok, PLAIN + ROT), BF), ((tok, 4 * slots), BF)], vm(2) + hb(4), 63.9,
        [
            pltpu.VMEM((PLAIN + ROT, tok), BF), pltpu.VMEM((2, tok), jnp.int32), pltpu.VMEM((GROUPS, tok), F32),
            pltpu.VMEM((2, tok), F32), pltpu.SemaphoreType.DMA((4,)),
        ],
    )(cos, sin, queries.T, expert_pick.T, group_logits.T, inner_logits.T)
    qs = [q_own] + [
        lax.ppermute(q_own, "x", [(i, (i + k) % xs) for i in range(xs)]) for k in range(1, xs)
    ]
    arrived, qs = lax.optimization_barrier((arrived, qs))
    into = pltpu.VMEM((width, 2 * ff), BF)
    hid, kv_all, down, down2 = call(
        hidden_kernel, "hidden",
        [((slots, 2 * ff), BF), ((slots, kv_w), BF), ((ff, width // 2), BF), ((ff, width // 2), BF)], SM + hb(7), 32,
        [pltpu.VMEM((slots, width + kv_w), BF), into, into, pltpu.SemaphoreType.DMA((5 + 2 * ys,))],
    )(cs, arrived.reshape(slots, width + kv_w), wg, wu, wg2, wu2, wd, wd2)
    hid2 = lax.ppermute(hid, "c", swap)
    (result,) = call(down_kernel, "down", [((experts, 2, half, width // 2), BF)], SM + vm(4), 24)(
        cs, hid, hid2, down, down2
    )
    returned = lax.all_to_all(result.reshape(experts, 2 * half, width // 2), ep, 0, 0, tiled=True)
    parts = call(attend_kernel, "attend", [((tok, 128), BF)] * xs, SM + vm(5), 16)(where, *qs, kv_all)
    back = [parts[0]] + [
        lax.ppermute(parts[k], "x", [(i, (i - k) % xs) for i in range(xs)]) for k in range(1, xs)
    ]
    keep_mix, send_mix = call(
        mix_kernel, "mix", [((ys, 8, width), BF)] * 2, SM + vm(5), 16, [pltpu.VMEM((tok, width), F32)]
    )(where, *back, w_out)
    got_mix = lax.ppermute(send_mix, "c", swap)
    mix_half = (keep_mix.astype(F32) + got_mix.astype(F32)).astype(BF)
    mix_rows = mix_half.reshape(ys, 8, width // 128, 128).transpose(0, 2, 1, 3).reshape(ys, width // 16, 128)

    returned, mix_rows = lax.optimization_barrier((returned, mix_rows))
    (partial_sums,) = call(combine_kernel, "combine", [((ys, 2 * tok, 128), BF)], vm(3), 16)(
        returned.reshape(2 * slots, width // 2), spread, mix_rows
    )
    last = lax.all_to_all(partial_sums, "y", 0, 0, tiled=True)
    summed = jnp.sum(last.astype(F32), axis=0).astype(BF)
    expert_out = summed[:tok]
    mixer_out = summed[tok:].reshape(width // 128, 8, 128).transpose(1, 0, 2).reshape(8, width)
    return mixer_out, expert_out


def solution(mesh):
    fine = Mesh(mesh.devices.reshape(8, 4, 8, 2), ("z", "x", "y", "c"))
    e, t = ("z", "x"), ("y", "c")
    in_specs = (
        P(e, t), P(e, None), P(e, None), P(), P(None, t), P(t, None), P(e, None), P(),
        P(e, None), P(e, None), P(e, None), P(e, None, t), P(e, None, t), P(e, t, None),
    )
    out_specs = (P(e + t, None), P(e, t))
    return jax.shard_map(per_device, mesh=fine, in_specs=in_specs, out_specs=out_specs, check_vma=False)
```

```python
import functools

import jax
import jax.numpy as jnp
import numpy as np
from jax import lax
from jax.experimental import pallas as pl
from jax.experimental.pallas import tpu as pltpu
from jax.sharding import Mesh, PartitionSpec as P

PLAIN = 64
ROT = 32
VAL = 64
SEG = 64
GROUPS = 4
BF = jnp.bfloat16
F32 = jnp.float32
MIB = 1024 * 1024


def turn(v, cos, sin):
    a, b = v[: ROT // 2].astype(F32), v[ROT // 2 :].astype(F32)
    return jnp.concatenate([a * cos - b * sin, b * cos + a * sin], axis=0)


def fetch(pairs, sems):
    copies = [pltpu.make_async_copy(src, dst, sems.at[i]) for i, (src, dst) in enumerate(pairs)]
    for cp in copies:
        cp.start()
    return copies


def choose(pick_ref, experts, base, count):
    tok = pick_ref.shape[1]
    eid = lax.broadcasted_iota(jnp.int32, (experts, tok), 0)
    hit0, hit1 = eid == pick_ref[0:1, :], eid == pick_ref[1:2, :]
    hit = hit0 | hit1
    before = lax.broadcasted_iota(jnp.int32, (tok, tok), 0) < lax.broadcasted_iota(jnp.int32, (tok, tok), 1)
    rank = jnp.dot(
        jnp.where(hit, 1.0, 0.0).astype(BF), jnp.where(before, 1.0, 0.0).astype(BF), preferred_element_type=F32
    )
    code = jnp.where(hit, rank, -1.0)
    slot = (lax.broadcasted_iota(jnp.int32, (count, tok), 0) + base).astype(F32)
    sel = jnp.concatenate([jnp.where(code[e : e + 1, :] == slot, 1.0, 0.0) for e in range(experts)], axis=0)
    return hit0, hit1, sel


def rows_kernel(
    where_ref, cos_hbm, sin_hbm, tok_hbm, gain_hbm, pick_hbm, lat_hbm, lgain_hbm, up_hbm, rot_hbm,
    o_ref, cos_ref, sin_ref, tok_ref, gain_ref, pick_ref, lat_ref, lgain_ref, up_ref, rot_ref, sems,
):
    own = where_ref[4]
    cps = fetch((
        (pick_hbm, pick_ref), (lat_hbm, lat_ref), (lgain_hbm, lgain_ref), (up_hbm, up_ref), (rot_hbm, rot_ref),
        (cos_hbm.at[own], cos_ref), (sin_hbm.at[own], sin_ref), (tok_hbm, tok_ref), (gain_hbm, gain_ref),
    ), sems)
    half = tok_ref.shape[1] // 2
    experts = o_ref.shape[0] // 8
    cps[0].wait()
    _, _, sel = choose(pick_ref, experts, 8 * where_ref[2], 8)
    for cp in cps[1:7]:
        cp.wait()
    lat = lat_ref[...].astype(F32)
    lat = (lat * lax.rsqrt(jnp.mean(lat * lat, axis=1, keepdims=True) + 1e-06) * lgain_ref[...]).astype(BF)
    kv = jnp.dot(lat, up_ref[...], preferred_element_type=F32)
    rot = turn(rot_ref[...], cos_ref[...], sin_ref[...]).T
    blocks = []
    for q in range(4):
        rows = [slice(32 * q + 8 * i, 32 * q + 8 * i + 8) for i in range(4)]
        blocks.append(jnp.concatenate([kv[r] for r in rows] + [rot[r] for r in rows], axis=1).astype(BF))
    for e in range(experts):
        o_ref[8 * e : 8 * e + 8, half:] = blocks[e % 4]
    cps[7].wait()
    cps[8].wait()
    vals = tok_ref[...].astype(F32)
    mean = jnp.mean(vals, axis=1, keepdims=True)
    cen = vals - mean
    var = jnp.mean(cen * cen, axis=1, keepdims=True)
    cols = pl.ds(pl.multiple_of(half * where_ref[3], 128), half)
    cen = tok_ref[:, cols].astype(F32) - mean
    normed = (cen * lax.rsqrt(var + 1e-05) * gain_ref[:, cols]).astype(BF)
    o_ref[:, :half] = jnp.dot(sel.astype(BF), normed, preferred_element_type=F32).astype(BF)


def query_kernel(where_ref, cos_hbm, sin_hbm, q_hbm, q_out, cos_ref, sin_ref, q_ref, sems):
    own = where_ref[4]
    for cp in fetch(((cos_hbm.at[own], cos_ref), (sin_hbm.at[own], sin_ref), (q_hbm, q_ref)), sems):
        cp.wait()
    q = jnp.concatenate([q_ref[:PLAIN].astype(F32), turn(q_ref[PLAIN:], cos_ref[...], sin_ref[...])], axis=0)
    q_out[...] = q.T.astype(BF)


def spread_kernel(pick_ref, gl_ref, il_ref, w_ref):
    experts = w_ref.shape[1] // 32
    tok = w_ref.shape[0]
    hit0, hit1, sel = choose(pick_ref, experts, 0, 16)
    gl = gl_ref[...]
    home = pick_ref[0:1, :] // (experts // GROUPS)
    gid = lax.broadcasted_iota(jnp.int32, (GROUPS, tok), 0)
    own = jnp.sum(jnp.where(gid == home, gl, 0.0), axis=0, keepdims=True)
    share = 1.0 / jnp.sum(jnp.exp(gl - own), axis=0, keepdims=True)
    gap = il_ref[0:1, :] - il_ref[1:2, :]
    first = share * (1.0 / (1.0 + jnp.exp(-gap)))
    second = share * (1.0 / (1.0 + jnp.exp(gap)))
    weight = jnp.where(hit0, first, 0.0) + jnp.where(hit1, second, 0.0)
    spread = sel * jnp.concatenate([jnp.broadcast_to(weight[e : e + 1, :], (16, tok)) for e in range(experts)], axis=0)
    hi = spread.astype(BF).astype(F32)
    w_ref[...] = jnp.concatenate([hi, spread - hi], axis=0).T.astype(BF)


def split3(v):
    hi = v.astype(BF).astype(F32)
    rest = v - hi
    mid = rest.astype(BF).astype(F32)
    return hi, mid, rest - mid


def attend_kernel(where_ref, q0, q1, q2, q3, kv_ref, o0, o1, o2, o3):
    z, x = where_ref[0], where_ref[1]
    xs = 4
    tok = q0.shape[0]
    segs = tok // SEG
    count = kv_ref.shape[0]
    base = 4 * (PLAIN + VAL)
    keys = jnp.concatenate([
        jnp.concatenate([kv_ref[:, 128 * i : 128 * i + PLAIN], kv_ref[:, base + ROT * i : base + ROT * i + ROT]], axis=1)
        for i in range(4)
    ], axis=0)
    vals = jnp.concatenate([kv_ref[:, 128 * i + PLAIN : 128 * i + 128] for i in range(4)], axis=0)
    col = lax.broadcasted_iota(jnp.int32, (1, 4 * count), 1)
    part = (tok // xs) * x + 8 * (col // count) + col % 8
    key_seg = ((col % count) // 8) * segs + part // SEG
    row = lax.broadcasted_iota(jnp.int32, (tok, 1), 0)
    scale = (PLAIN + ROT) ** -0.5
    lane = lax.broadcasted_iota(jnp.int32, (tok, 128), 1)
    for k, (q_ref, o_ref) in enumerate(((q0, o0), (q1, o1), (q2, o2), (q3, o3))):
        xq = lax.rem(x + xs - k, xs)
        q_seg = (z * xs + xq) * segs + row // SEG
        s = lax.dot_general(q_ref[...], keys, (((1,), (1,)), ((), ())), preferred_element_type=F32) * scale
        s = jnp.where(q_seg >= key_seg, s, -3e38)
        m = jnp.maximum(jnp.max(s, axis=1, keepdims=True), -1e30)
        p = jnp.exp(s - m)
        l = jnp.sum(p, axis=1, keepdims=True)
        acc = jnp.dot(p.astype(BF), vals, preferred_element_type=F32)
        out = jnp.concatenate([acc, jnp.zeros((tok, 128 - VAL), F32)], axis=1)
        for i, piece in enumerate(split3(m) + split3(l)):
            out = jnp.where(lane == VAL + i, piece, out)
        o_ref[...] = out.astype(BF)


def mix_kernel(where_ref, a0, a1, a2, a3, w_ref, keep_ref, send_ref, res_ref):
    c = where_ref[2]
    parts = [r[...].astype(F32) for r in (a0, a1, a2, a3)]
    ms = [p[:, VAL : VAL + 1] + p[:, VAL + 1 : VAL + 2] + p[:, VAL + 2 : VAL + 3] for p in parts]
    ls = [p[:, VAL + 3 : VAL + 4] + p[:, VAL + 4 : VAL + 5] + p[:, VAL + 5 : VAL + 6] for p in parts]
    m = functools.reduce(jnp.maximum, ms)
    total = denom = 0.0
    for p, mp, lp in zip(parts, ms, ls):
        w = jnp.exp(mp - m)
        total = total + w * p[:, :VAL]
        denom = denom + w * lp
    attended = (total / denom).astype(BF)
    res_ref[...] = jnp.dot(attended, w_ref[...], preferred_element_type=F32)
    for y in range(keep_ref.shape[0]):
        keep_ref[y] = res_ref[pl.ds(pl.multiple_of(16 * y + 8 * c, 8), 8), :].astype(BF)
        send_ref[y] = res_ref[pl.ds(pl.multiple_of(16 * y + 8 * (1 - c), 8), 8), :].astype(BF)


def weight_pairs(refs, gu, base):
    f = refs[0].shape[1]
    rows = pl.ds(pl.multiple_of(base, 8), gu.shape[0])
    return [(r.at[rows, :], gu.at[:, i * f : (i + 1) * f]) for i, r in enumerate(refs)]


def first_kernel(where_ref, xh, g0h, u0h, g1h, u1h, pre_ref, kv_ref, x_ref, gu, sems):
    half = gu.shape[0]
    cps = fetch([(xh, x_ref)] + weight_pairs((g0h, u0h, g1h, u1h), gu, half * where_ref[3]), sems)
    cps[0].wait()
    kv_ref[...] = x_ref[:, half:]
    for cp in cps[1:]:
        cp.wait()
    pre_ref[...] = jnp.dot(x_ref[:, :half], gu[...], preferred_element_type=F32)


def second_kernel(where_ref, lo_ref, hi_ref, pre_ref, g0h, u0h, g1h, u1h, dh, d2h, o_ref, d, d2, gu, sems):
    c = where_ref[2]
    half = gu.shape[0]
    f = o_ref.shape[1] // 2
    pairs = weight_pairs((g0h, u0h, g1h, u1h), gu, half * (1 - where_ref[3]))
    for y in range(d.shape[1] // 128):
        cols = pl.ds(pl.multiple_of(128 * (2 * y + c), 128), 128)
        pairs += [(dh.at[:, cols], d.at[:, 128 * y : 128 * y + 128]), (d2h.at[:, cols], d2.at[:, 128 * y : 128 * y + 128])]
    cps = fetch(pairs, sems)
    rows = jnp.concatenate([lo_ref[...], hi_ref[...]], axis=1)
    for i in range(2):
        cps[2 * i].wait()
        cps[2 * i + 1].wait()
        cols = slice(2 * i * f, 2 * (i + 1) * f)
        both = pre_ref[:, cols] + jnp.dot(rows, gu[:, cols], preferred_element_type=F32)
        g, u = both[:, :f], both[:, f:]
        o_ref[:, i * f : (i + 1) * f] = (g / (1.0 + jnp.exp(-g)) * u).astype(BF)
    for cp in cps[4:]:
        cp.wait()


def down_kernel(c_ref, h_ref, h2_ref, d, d2, o_ref):
    c = c_ref[0]
    f = d.shape[0]
    for i, h, first, second in ((c, h_ref, d, d2), (1 - c, h2_ref, d2, d)):
        acc = jnp.dot(h[:, :f], first[...], preferred_element_type=F32) + jnp.dot(
            h[:, f:], second[...], preferred_element_type=F32
        )
        o_ref[:, pl.ds(i, 1)] = acc.astype(BF).reshape(o_ref.shape[0], 1, o_ref.shape[2], o_ref.shape[3])


def combine_kernel(r_ref, w_ref, mix_ref, o_ref):
    tok = w_ref.shape[0]
    both = jnp.concatenate([r_ref[...], r_ref[...]], axis=0)
    out = jnp.dot(w_ref[...], both, preferred_element_type=F32)
    for y in range(o_ref.shape[0]):
        o_ref[y, :tok] = out[:, 128 * y : 128 * (y + 1)].astype(BF)
        o_ref[y, tok:] = mix_ref[y]


def vm(n):
    return [pl.BlockSpec(memory_space=pltpu.VMEM)] * n


def hb(n):
    return [pl.BlockSpec(memory_space=pltpu.HBM)] * n


SM = [pl.BlockSpec(memory_space=pltpu.SMEM)]


def call(kernel, name, outs, ins, mib, scratch=()):
    return pl.pallas_call(
        kernel,
        out_shape=[jax.ShapeDtypeStruct(shape, dtype) for shape, dtype in outs],
        in_specs=ins,
        out_specs=vm(len(outs)),
        scratch_shapes=list(scratch),
        cost_estimate=pl.CostEstimate(flops=1000000, bytes_accessed=0, transcendentals=0),
        name=name,
        compiler_params=pltpu.CompilerParams(vmem_limit_bytes=int(mib * MIB)),
    )


def per_device(
    queries, token_latents, key_rotary, latent_norm_gain, latent_up_weight, w_out,
    tokens_b, moe_gain, group_logits, inner_logits, expert_pick, w_gate, w_up, w_down,
):
    ep = ("z", "x")
    zs, xs, ys = lax.axis_size("z"), lax.axis_size("x"), lax.axis_size("y")
    z, x, c = (lax.axis_index(n).astype(jnp.int32) for n in ("z", "x", "c"))
    tok = queries.shape[0]
    width = tokens_b.shape[1]
    experts = zs * xs
    half = 8
    slots = experts * half
    ff = w_gate.shape[2]
    swap = [(0, 1), (1, 0)]

    freq = 10000.0 ** (-np.arange(ROT // 2) * 2.0 / ROT)
    ang = freq[None, :, None] * np.arange(experts * tok).reshape(experts, 1, tok)
    cos, sin = jnp.asarray(np.cos(ang), F32), jnp.asarray(np.sin(ang), F32)
    table = pltpu.VMEM((ROT // 2, tok), F32)

    y = lax.axis_index("y").astype(jnp.int32)
    where = jnp.stack([z, x, c, y % 2, z * xs + x])
    lat_w = token_latents.shape[1]
    cols = width // 2
    kv_w = (tok // xs // 8) * (PLAIN + ROT + VAL)
    (outbound,) = call(
        rows_kernel, "rows", [((slots, cols + kv_w), BF)], SM + hb(9), 63.9,
        [
            table, table, pltpu.VMEM((tok, width), BF), pltpu.VMEM((1, width), F32), pltpu.VMEM((2, tok), jnp.int32),
            pltpu.VMEM((tok, lat_w), BF), pltpu.VMEM((1, lat_w), F32), pltpu.VMEM((lat_w, PLAIN + VAL), BF),
            pltpu.VMEM((ROT, tok), BF), pltpu.SemaphoreType.DMA((9,)),
        ],
    )(
        where, cos, sin, tokens_b, moe_gain[None, :], expert_pick.T, token_latents, latent_norm_gain[None, :],
        latent_up_weight, key_rotary.T,
    )
    arrived = lax.all_to_all(outbound.reshape(experts, half, cols + kv_w), ep, 0, 0, tiled=True)

    wg, wu, wd = w_gate[0], w_up[0], w_down[0]
    wg2, wu2, wd2 = (lax.ppermute(w, "c", swap) for w in (wg, wu, wd))

    (q_own,) = call(
        query_kernel, "query", [((tok, PLAIN + ROT), BF)], SM + hb(3), 63.9,
        [table, table, pltpu.VMEM((PLAIN + ROT, tok), BF), pltpu.SemaphoreType.DMA((3,))],
    )(where, cos, sin, queries.T)
    qs = [q_own] + [
        lax.ppermute(q_own, "x", [(i, (i + k) % xs) for i in range(xs)]) for k in range(1, xs)
    ]
    arrived, qs = lax.optimization_barrier((arrived, qs))
    arrived = arrived.reshape(slots, cols + kv_w)
    low = lax.ppermute(arrived[:, : cols // 2], "y", [(i, (i + 1) % ys) for i in range(ys)])
    high = lax.ppermute(arrived[:, cols // 2 : cols], "y", [(i, (i - 1) % ys) for i in range(ys)])
    into = pltpu.VMEM((cols, 4 * ff), BF)
    pre, kv_all = call(
        first_kernel, "first", [((slots, 4 * ff), F32), ((slots, kv_w), BF)], SM + hb(5), 32,
        [pltpu.VMEM((slots, cols + kv_w), BF), into, pltpu.SemaphoreType.DMA((5,))],
    )(where, arrived, wg, wu, wg2, wu2)
    hid, down, down2 = call(
        second_kernel, "second", [((slots, 2 * ff), BF), ((ff, cols), BF), ((ff, cols), BF)], SM + vm(3) + hb(6), 32,
        [into, pltpu.SemaphoreType.DMA((4 + 2 * ys,))],
    )(where, low, high, pre, wg, wu, wg2, wu2, wd, wd2)
    hid2 = lax.ppermute(hid, "c", swap)
    (result,) = call(down_kernel, "down", [((experts, 2, half, cols), BF)], SM + vm(4), 24)(
        c.reshape(1), hid, hid2, down, down2
    )
    pick_in, group_in, inner_in, _ = lax.optimization_barrier((expert_pick.T, group_logits.T, inner_logits.T, result))
    (spread,) = call(spread_kernel, "spread", [((tok, 4 * slots), BF)], vm(3), 16)(pick_in, group_in, inner_in)
    returned = lax.all_to_all(result.reshape(experts, 2 * half, width // 2), ep, 0, 0, tiled=True)
    parts = call(attend_kernel, "attend", [((tok, 128), BF)] * xs, SM + vm(5), 16)(where, *qs, kv_all)
    back = [parts[0]] + [
        lax.ppermute(parts[k], "x", [(i, (i - k) % xs) for i in range(xs)]) for k in range(1, xs)
    ]
    keep_mix, send_mix = call(
        mix_kernel, "mix", [((ys, 8, width), BF)] * 2, SM + vm(5), 16, [pltpu.VMEM((tok, width), F32)]
    )(where, *back, w_out)
    got_mix = lax.ppermute(send_mix, "c", swap)
    mix_half = (keep_mix.astype(F32) + got_mix.astype(F32)).astype(BF)
    mix_rows = mix_half.reshape(ys, 8, width // 128, 128).transpose(0, 2, 1, 3).reshape(ys, width // 16, 128)

    returned, mix_rows = lax.optimization_barrier((returned, mix_rows))
    (partial_sums,) = call(combine_kernel, "combine", [((ys, 2 * tok, 128), BF)], vm(3), 16)(
        returned.reshape(2 * slots, width // 2), spread, mix_rows
    )
    last = lax.all_to_all(partial_sums, "y", 0, 0, tiled=True)
    summed = jnp.sum(last.astype(F32), axis=0).astype(BF)
    expert_out = summed[:tok]
    mixer_out = summed[tok:].reshape(width // 128, 8, 128).transpose(1, 0, 2).reshape(8, width)
    return mixer_out, expert_out


def solution(mesh):
    fine = Mesh(mesh.devices.reshape(8, 4, 8, 2), ("z", "x", "y", "c"))
    e, t = ("z", "x"), ("y", "c")
    in_specs = (
        P(e, t), P(e, None), P(e, None), P(), P(None, t), P(t, None), P(e, None), P(),
        P(e, None), P(e, None), P(e, None), P(e, None, t), P(e, None, t), P(e, t, None),
    )
    out_specs = (P(e + t, None), P(e, t))
    return jax.shard_map(per_device, mesh=fine, in_specs=in_specs, out_specs=out_specs, check_vma=False)
```

```python
import functools

import jax
import jax.numpy as jnp
from jax import lax
from jax.experimental import pallas as pl
from jax.experimental.pallas import tpu as pltpu
from jax.sharding import Mesh, PartitionSpec as P

PLAIN = 64
ROT = 32
VAL = 64
SEG = 64
GROUPS = 4
BF = jnp.bfloat16
F32 = jnp.float32
MIB = 1024 * 1024


def turn(v, cos, sin):
    a, b = v[: ROT // 2].astype(F32), v[ROT // 2 :].astype(F32)
    return jnp.concatenate([a * cos - b * sin, b * cos + a * sin], axis=0)


def fetch(pairs, sems):
    copies = [pltpu.make_async_copy(src, dst, sems.at[i]) for i, (src, dst) in enumerate(pairs)]
    for cp in copies:
        cp.start()
    return copies


def choose(pick_ref, experts, base, count):
    tok = pick_ref.shape[1]
    eid = lax.broadcasted_iota(jnp.int32, (experts, tok), 0)
    hit0, hit1 = eid == pick_ref[0:1, :], eid == pick_ref[1:2, :]
    hit = hit0 | hit1
    before = lax.broadcasted_iota(jnp.int32, (tok, tok), 0) < lax.broadcasted_iota(jnp.int32, (tok, tok), 1)
    rank = jnp.dot(
        jnp.where(hit, 1.0, 0.0).astype(BF), jnp.where(before, 1.0, 0.0).astype(BF), preferred_element_type=F32
    )
    code = jnp.where(hit, rank, -1.0)
    slot = (lax.broadcasted_iota(jnp.int32, (count, tok), 0) + base).astype(F32)
    sel = jnp.concatenate([jnp.where(code[e : e + 1, :] == slot, 1.0, 0.0) for e in range(experts)], axis=0)
    return hit0, hit1, sel


def keys_kernel(
    lat_hbm, rot_hbm, cos_ref, sin_ref, gain_hbm, up_hbm, pick_hbm, gl_hbm, il_hbm,
    o_ref, w_ref, lat_ref, rot_ref, gain_ref, up_ref, pick_ref, gl_ref, il_ref, sems,
):
    pairs = (
        (lat_hbm, lat_ref), (gain_hbm, gain_ref), (up_hbm, up_ref), (rot_hbm, rot_ref),
        (pick_hbm, pick_ref), (gl_hbm, gl_ref), (il_hbm, il_ref),
    )
    for cp in fetch(pairs, sems):
        cp.wait()
    lat = lat_ref[...].astype(F32)
    lat = (lat * lax.rsqrt(jnp.mean(lat * lat, axis=1, keepdims=True) + 1e-06) * gain_ref[...]).astype(BF)
    kv = jnp.dot(lat, up_ref[...], preferred_element_type=F32).T
    rot = turn(rot_ref[...], cos_ref[...], sin_ref[...])
    pack = jnp.concatenate([kv[:PLAIN], rot, kv[PLAIN:]], axis=0).astype(BF)
    for b in range(o_ref.shape[0]):
        o_ref[b] = pack

    experts = w_ref.shape[1] // 32
    tok = w_ref.shape[0]
    hit0, hit1, sel = choose(pick_ref, experts, 0, 16)
    gl = gl_ref[...]
    home = pick_ref[0:1, :] // (experts // GROUPS)
    gid = lax.broadcasted_iota(jnp.int32, (GROUPS, tok), 0)
    own = jnp.sum(jnp.where(gid == home, gl, 0.0), axis=0, keepdims=True)
    share = 1.0 / jnp.sum(jnp.exp(gl - own), axis=0, keepdims=True)
    gap = il_ref[0:1, :] - il_ref[1:2, :]
    first = share * (1.0 / (1.0 + jnp.exp(-gap)))
    second = share * (1.0 / (1.0 + jnp.exp(gap)))
    weight = jnp.where(hit0, first, 0.0) + jnp.where(hit1, second, 0.0)
    spread = sel * jnp.concatenate([jnp.broadcast_to(weight[e : e + 1, :], (16, tok)) for e in range(experts)], axis=0)
    hi = spread.astype(BF).astype(F32)
    w_ref[...] = jnp.concatenate([hi, spread - hi], axis=0).T.astype(BF)


def rows_kernel(c_ref, tok_hbm, gain_hbm, pick_hbm, o_ref, tok_ref, gain_ref, pick_ref, sems):
    cps = fetch(((pick_hbm, pick_ref), (tok_hbm, tok_ref), (gain_hbm, gain_ref)), sems)
    cps[0].wait()
    _, _, sel = choose(pick_ref, o_ref.shape[0] // 8, 8 * c_ref[0], 8)
    cps[1].wait()
    cps[2].wait()
    vals = tok_ref[...].astype(F32)
    cen = vals - jnp.mean(vals, axis=1, keepdims=True)
    var = jnp.mean(cen * cen, axis=1, keepdims=True)
    normed = (cen * lax.rsqrt(var + 1e-05) * gain_ref[...]).astype(BF)
    o_ref[...] = jnp.dot(sel.astype(BF), normed, preferred_element_type=F32).astype(BF)


def split3(v):
    hi = v.astype(BF).astype(F32)
    rest = v - hi
    mid = rest.astype(BF).astype(F32)
    return hi, mid, rest - mid


def query_kernel(q_ref, cos_ref, sin_ref, o_ref):
    q = jnp.concatenate([q_ref[:PLAIN].astype(F32), turn(q_ref[PLAIN:], cos_ref[...], sin_ref[...])], axis=0)
    o_ref[...] = q.T.astype(BF)


def attend_kernel(where_ref, q0, q1, q2, q3, kv_ref, o0, o1, o2, o3):
    z, x = where_ref[0], where_ref[1]
    xs = 4
    zs, _, tok = kv_ref.shape
    segs = tok // SEG
    keys = jnp.concatenate([kv_ref[b, : PLAIN + ROT, :] for b in range(zs)], axis=1)
    vals = jnp.concatenate([kv_ref[b, PLAIN + ROT :, :] for b in range(zs)], axis=1)
    col = lax.broadcasted_iota(jnp.int32, (1, zs * tok), 1)
    key_seg = ((col // tok) * xs + x) * segs + (col % tok) // SEG
    row = lax.broadcasted_iota(jnp.int32, (tok, 1), 0)
    scale = (PLAIN + ROT) ** -0.5
    lane = lax.broadcasted_iota(jnp.int32, (tok, 128), 1)
    for k, (q_ref, o_ref) in enumerate(((q0, o0), (q1, o1), (q2, o2), (q3, o3))):
        xq = lax.rem(x + xs - k, xs)
        q_seg = (z * xs + xq) * segs + row // SEG
        s = jnp.dot(q_ref[...], keys, preferred_element_type=F32) * scale
        s = jnp.where(q_seg >= key_seg, s, -3e38)
        m = jnp.maximum(jnp.max(s, axis=1, keepdims=True), -1e30)
        p = jnp.exp(s - m)
        l = jnp.sum(p, axis=1, keepdims=True)
        acc = lax.dot_general(p.astype(BF), vals, (((1,), (1,)), ((), ())), preferred_element_type=F32)
        out = jnp.concatenate([acc, jnp.zeros((tok, 128 - VAL), F32)], axis=1)
        for i, piece in enumerate(split3(m) + split3(l)):
            out = jnp.where(lane == VAL + i, piece, out)
        o_ref[...] = out.astype(BF)


def mix_kernel(where_ref, a0, a1, a2, a3, w_ref, keep_ref, send_ref, res_ref):
    c = where_ref[2]
    parts = [r[...].astype(F32) for r in (a0, a1, a2, a3)]
    ms = [p[:, VAL : VAL + 1] + p[:, VAL + 1 : VAL + 2] + p[:, VAL + 2 : VAL + 3] for p in parts]
    ls = [p[:, VAL + 3 : VAL + 4] + p[:, VAL + 4 : VAL + 5] + p[:, VAL + 5 : VAL + 6] for p in parts]
    m = functools.reduce(jnp.maximum, ms)
    total = denom = 0.0
    for p, mp, lp in zip(parts, ms, ls):
        w = jnp.exp(mp - m)
        total = total + w * p[:, :VAL]
        denom = denom + w * lp
    attended = (total / denom).astype(BF)
    res_ref[...] = jnp.dot(attended, w_ref[...], preferred_element_type=F32)
    for y in range(keep_ref.shape[0]):
        keep_ref[y] = res_ref[pl.ds(pl.multiple_of(16 * y + 8 * c, 8), 8), :].astype(BF)
        send_ref[y] = res_ref[pl.ds(pl.multiple_of(16 * y + 8 * (1 - c), 8), 8), :].astype(BF)


def hidden_kernel(c_ref, xh, g0h, u0h, g1h, u1h, dh, d2h, o_ref, d, d2, x_ref, gu0, gu1, sems):
    c = c_ref[0]
    f = o_ref.shape[1] // 2
    pairs = [(xh, x_ref), (g0h, gu0.at[:, :f]), (u0h, gu0.at[:, f:]), (g1h, gu1.at[:, :f]), (u1h, gu1.at[:, f:])]
    for y in range(d.shape[1] // 128):
        cols = pl.ds(pl.multiple_of(128 * (2 * y + c), 128), 128)
        pairs += [(dh.at[:, cols], d.at[:, 128 * y : 128 * y + 128]), (d2h.at[:, cols], d2.at[:, 128 * y : 128 * y + 128])]
    cps = fetch(pairs, sems)
    cps[0].wait()
    rows = x_ref[...]
    for i, gu_ref in enumerate((gu0, gu1)):
        cps[2 * i + 1].wait()
        cps[2 * i + 2].wait()
        both = jnp.dot(rows, gu_ref[...], preferred_element_type=F32)
        g, u = both[:, :f], both[:, f:]
        o_ref[:, i * f : (i + 1) * f] = (g / (1.0 + jnp.exp(-g)) * u).astype(BF)
    for cp in cps[5:]:
        cp.wait()


def down_kernel(c_ref, h_ref, h2_ref, d, d2, o_ref):
    c = c_ref[0]
    f = d.shape[0]
    for i, h, first, second in ((c, h_ref, d, d2), (1 - c, h2_ref, d2, d)):
        acc = jnp.dot(h[:, :f], first[...], preferred_element_type=F32) + jnp.dot(
            h[:, f:], second[...], preferred_element_type=F32
        )
        o_ref[:, pl.ds(i, 1)] = acc.astype(BF).reshape(o_ref.shape[0], 1, o_ref.shape[2], o_ref.shape[3])


def combine_kernel(r_ref, w_ref, mix_ref, o_ref):
    tok = w_ref.shape[0]
    both = jnp.concatenate([r_ref[...], r_ref[...]], axis=0)
    out = jnp.dot(w_ref[...], both, preferred_element_type=F32)
    for y in range(o_ref.shape[0]):
        o_ref[y, :tok] = out[:, 128 * y : 128 * (y + 1)].astype(BF)
        o_ref[y, tok:] = mix_ref[y]


def vm(n):
    return [pl.BlockSpec(memory_space=pltpu.VMEM)] * n


def hb(n):
    return [pl.BlockSpec(memory_space=pltpu.HBM)] * n


SM = [pl.BlockSpec(memory_space=pltpu.SMEM)]


def call(kernel, name, outs, ins, mib, scratch=()):
    return pl.pallas_call(
        kernel,
        out_shape=[jax.ShapeDtypeStruct(shape, dtype) for shape, dtype in outs],
        in_specs=ins,
        out_specs=vm(len(outs)),
        scratch_shapes=list(scratch),
        cost_estimate=pl.CostEstimate(flops=1000000, bytes_accessed=0, transcendentals=0),
        name=name,
        compiler_params=pltpu.CompilerParams(vmem_limit_bytes=int(mib * MIB)),
    )


def per_device(
    queries, token_latents, key_rotary, latent_norm_gain, latent_up_weight, w_out,
    tokens_b, moe_gain, group_logits, inner_logits, expert_pick, w_gate, w_up, w_down,
):
    ep = ("z", "x")
    zs, xs, ys = lax.axis_size("z"), lax.axis_size("x"), lax.axis_size("y")
    z, x, c = (lax.axis_index(n).astype(jnp.int32) for n in ("z", "x", "c"))
    tok = queries.shape[0]
    width = tokens_b.shape[1]
    experts = zs * xs
    half = 8
    slots = experts * half
    ff = w_gate.shape[2]
    swap = [(0, 1), (1, 0)]

    positions = ((z * xs + x) * tok + jnp.arange(tok, dtype=jnp.int32)).astype(F32)
    freq = jnp.power(10000.0, -jnp.arange(ROT // 2, dtype=F32) * 2.0 / ROT)
    ang = freq[:, None] * positions[None, :]
    cos, sin = jnp.cos(ang), jnp.sin(ang)

    where = jnp.stack([z, x, c])
    cs = c.reshape(1)
    (outbound,) = call(
        rows_kernel, "rows", [((slots, width), BF)], SM + hb(3), 63.9,
        [
            pltpu.VMEM((tok, width), BF), pltpu.VMEM((1, width), F32), pltpu.VMEM((2, tok), jnp.int32),
            pltpu.SemaphoreType.DMA((3,)),
        ],
    )(cs, tokens_b, moe_gain[None, :], expert_pick.T)
    arrived = lax.all_to_all(outbound.reshape(experts, half, width), ep, 0, 0, tiled=True)

    wg, wu, wd = w_gate[0], w_up[0], w_down[0]
    wg2, wu2, wd2 = (lax.ppermute(w, "c", swap) for w in (wg, wu, wd))

    lat_w = token_latents.shape[1]
    pack, spread = call(
        keys_kernel, "keys", [((zs, PLAIN + ROT + VAL, tok), BF), ((tok, 4 * slots), BF)],
        hb(2) + vm(2) + hb(5), 63.9,
        [
            pltpu.VMEM((tok, lat_w), BF), pltpu.VMEM((ROT, tok), BF), pltpu.VMEM((1, lat_w), F32),
            pltpu.VMEM((lat_w, PLAIN + VAL), BF), pltpu.VMEM((2, tok), jnp.int32),
            pltpu.VMEM((GROUPS, tok), F32), pltpu.VMEM((2, tok), F32), pltpu.SemaphoreType.DMA((7,)),
        ],
    )(
        token_latents, key_rotary.T, cos, sin, latent_norm_gain[None, :], latent_up_weight,
        expert_pick.T, group_logits.T, inner_logits.T,
    )
    (q_own,) = call(query_kernel, "query", [((tok, PLAIN + ROT), BF)], vm(3), 63.9)(queries.T, cos, sin)
    qs = [q_own] + [
        lax.ppermute(q_own, "x", [(i, (i + k) % xs) for i in range(xs)]) for k in range(1, xs)
    ]
    arrived, pack, qs = lax.optimization_barrier((arrived, pack, qs))
    kv_all = lax.all_to_all(pack, "z", 0, 0, tiled=True)
    into = pltpu.VMEM((width, 2 * ff), BF)
    hid, down, down2 = call(
        hidden_kernel, "hidden", [((slots, 2 * ff), BF), ((ff, width // 2), BF), ((ff, width // 2), BF)],
        SM + hb(7), 32, [pltpu.VMEM((slots, width), BF), into, into, pltpu.SemaphoreType.DMA((5 + 2 * ys,))],
    )(cs, arrived.reshape(slots, width), wg, wu, wg2, wu2, wd, wd2)
    hid2 = lax.ppermute(hid, "c", swap)
    (result,) = call(down_kernel, "down", [((experts, 2, half, width // 2), BF)], SM + vm(4), 24)(
        cs, hid, hid2, down, down2
    )
    result, kv_all = lax.optimization_barrier((result, kv_all))
    returned = lax.all_to_all(result.reshape(experts, 2 * half, width // 2), ep, 0, 0, tiled=True)
    parts = call(attend_kernel, "attend", [((tok, 128), BF)] * xs, SM + vm(5), 16)(where, *qs, kv_all)
    back = [parts[0]] + [
        lax.ppermute(parts[k], "x", [(i, (i - k) % xs) for i in range(xs)]) for k in range(1, xs)
    ]
    keep_mix, send_mix = call(
        mix_kernel, "mix", [((ys, 8, width), BF)] * 2, SM + vm(5), 16, [pltpu.VMEM((tok, width), F32)]
    )(where, *back, w_out)
    got_mix = lax.ppermute(send_mix, "c", swap)
    mix_half = (keep_mix.astype(F32) + got_mix.astype(F32)).astype(BF)
    mix_rows = mix_half.reshape(ys, 8, width // 128, 128).transpose(0, 2, 1, 3).reshape(ys, width // 16, 128)

    returned, mix_rows = lax.optimization_barrier((returned, mix_rows))
    (partial_sums,) = call(combine_kernel, "combine", [((ys, 2 * tok, 128), BF)], vm(3), 16)(
        returned.reshape(2 * slots, width // 2), spread, mix_rows
    )
    last = lax.all_to_all(partial_sums, "y", 0, 0, tiled=True)
    summed = jnp.sum(last.astype(F32), axis=0).astype(BF)
    expert_out = summed[:tok]
    mixer_out = summed[tok:].reshape(width // 128, 8, 128).transpose(1, 0, 2).reshape(8, width)
    return mixer_out, expert_out


def solution(mesh):
    fine = Mesh(mesh.devices.reshape(8, 4, 8, 2), ("z", "x", "y", "c"))
    e, t = ("z", "x"), ("y", "c")
    in_specs = (
        P(e, t), P(e, None), P(e, None), P(), P(None, t), P(t, None), P(e, None), P(),
        P(e, None), P(e, None), P(e, None), P(e, None, t), P(e, None, t), P(e, t, None),
    )
    out_specs = (P(e + t, None), P(e, t))
    return jax.shard_map(per_device, mesh=fine, in_specs=in_specs, out_specs=out_specs, check_vma=False)
```

```python
import functools

import jax
import jax.numpy as jnp
from jax import lax
from jax.experimental import pallas as pl
from jax.experimental.pallas import tpu as pltpu
from jax.sharding import Mesh, PartitionSpec as P

PLAIN = 64
ROT = 32
VAL = 64
SEG = 64
GROUPS = 4
BF = jnp.bfloat16
F32 = jnp.float32
MIB = 1024 * 1024


def turn(v, cos, sin):
    a, b = v[: ROT // 2].astype(F32), v[ROT // 2 :].astype(F32)
    return jnp.concatenate([a * cos - b * sin, b * cos + a * sin], axis=0)


def fetch(pairs, sems):
    copies = [pltpu.make_async_copy(src, dst, sems.at[i]) for i, (src, dst) in enumerate(pairs)]
    for cp in copies:
        cp.start()
    return copies


def choose(pick_ref, experts, base, count):
    tok = pick_ref.shape[1]
    eid = lax.broadcasted_iota(jnp.int32, (experts, tok), 0)
    hit0, hit1 = eid == pick_ref[0:1, :], eid == pick_ref[1:2, :]
    hit = hit0 | hit1
    before = lax.broadcasted_iota(jnp.int32, (tok, tok), 0) < lax.broadcasted_iota(jnp.int32, (tok, tok), 1)
    rank = jnp.dot(
        jnp.where(hit, 1.0, 0.0).astype(BF), jnp.where(before, 1.0, 0.0).astype(BF), preferred_element_type=F32
    )
    code = jnp.where(hit, rank, -1.0)
    slot = (lax.broadcasted_iota(jnp.int32, (count, tok), 0) + base).astype(F32)
    sel = jnp.concatenate([jnp.where(code[e : e + 1, :] == slot, 1.0, 0.0) for e in range(experts)], axis=0)
    return hit0, hit1, sel


def keys_kernel(
    lat_hbm, rot_hbm, cos_ref, sin_ref, gain_hbm, up_hbm, pick_hbm, gl_hbm, il_hbm,
    o_ref, w_ref, lat_ref, rot_ref, gain_ref, up_ref, pick_ref, gl_ref, il_ref, sems,
):
    pairs = (
        (lat_hbm, lat_ref), (gain_hbm, gain_ref), (up_hbm, up_ref), (rot_hbm, rot_ref),
        (pick_hbm, pick_ref), (gl_hbm, gl_ref), (il_hbm, il_ref),
    )
    for cp in fetch(pairs, sems):
        cp.wait()
    lat = lat_ref[...].astype(F32)
    lat = (lat * lax.rsqrt(jnp.mean(lat * lat, axis=1, keepdims=True) + 1e-06) * gain_ref[...]).astype(BF)
    kv = jnp.dot(lat, up_ref[...], preferred_element_type=F32).T
    rot = turn(rot_ref[...], cos_ref[...], sin_ref[...])
    pack = jnp.concatenate([kv[:PLAIN], rot, kv[PLAIN:]], axis=0).astype(BF)
    for b in range(o_ref.shape[0]):
        o_ref[b] = pack

    experts = w_ref.shape[1] // 32
    tok = w_ref.shape[0]
    hit0, hit1, low = choose(pick_ref, experts, 0, 8)
    _, _, high = choose(pick_ref, experts, 8, 8)
    gl = gl_ref[...]
    home = pick_ref[0:1, :] // (experts // GROUPS)
    gid = lax.broadcasted_iota(jnp.int32, (GROUPS, tok), 0)
    own = jnp.sum(jnp.where(gid == home, gl, 0.0), axis=0, keepdims=True)
    share = 1.0 / jnp.sum(jnp.exp(gl - own), axis=0, keepdims=True)
    gap = il_ref[0:1, :] - il_ref[1:2, :]
    first = share * (1.0 / (1.0 + jnp.exp(-gap)))
    second = share * (1.0 / (1.0 + jnp.exp(gap)))
    weight = jnp.where(hit0, first, 0.0) + jnp.where(hit1, second, 0.0)
    each = jnp.concatenate([jnp.broadcast_to(weight[e : e + 1, :], (8, tok)) for e in range(experts)], axis=0)
    spread = jnp.concatenate([low * each, high * each], axis=0)
    hi = spread.astype(BF).astype(F32)
    w_ref[...] = jnp.concatenate([hi, spread - hi], axis=0).T.astype(BF)


def rows_kernel(c_ref, tok_hbm, gain_hbm, pick_hbm, o_ref, tok_ref, gain_ref, pick_ref, sems):
    cps = fetch(((pick_hbm, pick_ref), (tok_hbm, tok_ref), (gain_hbm, gain_ref)), sems)
    cps[0].wait()
    _, _, sel = choose(pick_ref, o_ref.shape[0] // 8, 8 * c_ref[0], 8)
    cps[1].wait()
    cps[2].wait()
    vals = tok_ref[...].astype(F32)
    cen = vals - jnp.mean(vals, axis=1, keepdims=True)
    var = jnp.mean(cen * cen, axis=1, keepdims=True)
    normed = (cen * lax.rsqrt(var + 1e-05) * gain_ref[...]).astype(BF)
    o_ref[...] = jnp.dot(sel.astype(BF), normed, preferred_element_type=F32).astype(BF)


def split3(v):
    hi = v.astype(BF).astype(F32)
    rest = v - hi
    mid = rest.astype(BF).astype(F32)
    return hi, mid, rest - mid


def query_kernel(q_ref, cos_ref, sin_ref, o_ref):
    q = jnp.concatenate([q_ref[:PLAIN].astype(F32), turn(q_ref[PLAIN:], cos_ref[...], sin_ref[...])], axis=0)
    o_ref[...] = q.T.astype(BF)


def attend_kernel(where_ref, q0, q1, q2, q3, kv_ref, o0, o1, o2, o3):
    z, x = where_ref[0], where_ref[1]
    xs = 4
    zs, _, tok = kv_ref.shape
    segs = tok // SEG
    keys = jnp.concatenate([kv_ref[b, : PLAIN + ROT, :] for b in range(zs)], axis=1)
    vals = jnp.concatenate([kv_ref[b, PLAIN + ROT :, :] for b in range(zs)], axis=1)
    col = lax.broadcasted_iota(jnp.int32, (1, zs * tok), 1)
    key_seg = ((col // tok) * xs + x) * segs + (col % tok) // SEG
    row = lax.broadcasted_iota(jnp.int32, (tok, 1), 0)
    scale = (PLAIN + ROT) ** -0.5
    lane = lax.broadcasted_iota(jnp.int32, (tok, 128), 1)
    for k, (q_ref, o_ref) in enumerate(((q0, o0), (q1, o1), (q2, o2), (q3, o3))):
        xq = lax.rem(x + xs - k, xs)
        q_seg = (z * xs + xq) * segs + row // SEG
        s = jnp.dot(q_ref[...], keys, preferred_element_type=F32) * scale
        s = jnp.where(q_seg >= key_seg, s, -3e38)
        m = jnp.maximum(jnp.max(s, axis=1, keepdims=True), -1e30)
        p = jnp.exp(s - m)
        l = jnp.sum(p, axis=1, keepdims=True)
        acc = lax.dot_general(p.astype(BF), vals, (((1,), (1,)), ((), ())), preferred_element_type=F32)
        out = jnp.concatenate([acc, jnp.zeros((tok, 128 - VAL), F32)], axis=1)
        for i, piece in enumerate(split3(m) + split3(l)):
            out = jnp.where(lane == VAL + i, piece, out)
        o_ref[...] = out.astype(BF)


def mix_kernel(where_ref, a0, a1, a2, a3, w_ref, keep_ref, send_ref, res_ref):
    c = where_ref[2]
    parts = [r[...].astype(F32) for r in (a0, a1, a2, a3)]
    ms = [p[:, VAL : VAL + 1] + p[:, VAL + 1 : VAL + 2] + p[:, VAL + 2 : VAL + 3] for p in parts]
    ls = [p[:, VAL + 3 : VAL + 4] + p[:, VAL + 4 : VAL + 5] + p[:, VAL + 5 : VAL + 6] for p in parts]
    m = functools.reduce(jnp.maximum, ms)
    total = denom = 0.0
    for p, mp, lp in zip(parts, ms, ls):
        w = jnp.exp(mp - m)
        total = total + w * p[:, :VAL]
        denom = denom + w * lp
    attended = (total / denom).astype(BF)
    res_ref[...] = jnp.dot(attended, w_ref[...], preferred_element_type=F32)
    for y in range(keep_ref.shape[0]):
        keep_ref[y] = res_ref[pl.ds(pl.multiple_of(16 * y + 8 * c, 8), 8), :].astype(BF)
        send_ref[y] = res_ref[pl.ds(pl.multiple_of(16 * y + 8 * (1 - c), 8), 8), :].astype(BF)


def hidden_kernel(c_ref, x_ref, g0h, u0h, g1h, u1h, dh, d2h, o_ref, d, d2, gu0, gu1, sems):
    c = c_ref[0]
    f = o_ref.shape[1] // 2
    pairs = [(g0h, gu0.at[:, :f]), (u0h, gu0.at[:, f:]), (g1h, gu1.at[:, :f]), (u1h, gu1.at[:, f:])]
    for y in range(d.shape[1] // 128):
        cols = pl.ds(pl.multiple_of(128 * (2 * y + c), 128), 128)
        pairs += [(dh.at[:, cols], d.at[:, 128 * y : 128 * y + 128]), (d2h.at[:, cols], d2.at[:, 128 * y : 128 * y + 128])]
    cps = fetch(pairs, sems)
    rows = x_ref[...]
    for i, gu_ref in enumerate((gu0, gu1)):
        cps[2 * i].wait()
        cps[2 * i + 1].wait()
        both = jnp.dot(rows, gu_ref[...], preferred_element_type=F32)
        g, u = both[:, :f], both[:, f:]
        o_ref[:, i * f : (i + 1) * f] = (g / (1.0 + jnp.exp(-g)) * u).astype(BF)
    for cp in cps[4:]:
        cp.wait()


def down_kernel(c_ref, h_ref, h2_ref, d, d2, o_ref):
    c = c_ref[0]
    f = d.shape[0]
    for i, h, first, second in ((c, h_ref, d, d2), (1 - c, h2_ref, d2, d)):
        acc = jnp.dot(h[:, :f], first[...], preferred_element_type=F32) + jnp.dot(
            h[:, f:], second[...], preferred_element_type=F32
        )
        wide = d.shape[1]
        o_ref[:, pl.ds(pl.multiple_of(wide * i, 128), wide)] = acc.astype(BF)


def combine_kernel(r_ref, w_ref, mix_ref, o_ref):
    tok = w_ref.shape[0]
    wide = r_ref.shape[1] // 2
    both = jnp.concatenate([r_ref[:, :wide], r_ref[:, wide:]] * 2, axis=0)
    out = jnp.dot(w_ref[...], both, preferred_element_type=F32)
    for y in range(o_ref.shape[0]):
        o_ref[y, :tok] = out[:, 128 * y : 128 * (y + 1)].astype(BF)
        o_ref[y, tok:] = mix_ref[y]


def vm(n):
    return [pl.BlockSpec(memory_space=pltpu.VMEM)] * n


def hb(n):
    return [pl.BlockSpec(memory_space=pltpu.HBM)] * n


SM = [pl.BlockSpec(memory_space=pltpu.SMEM)]


def call(kernel, name, outs, ins, mib, scratch=()):
    return pl.pallas_call(
        kernel,
        out_shape=[jax.ShapeDtypeStruct(shape, dtype) for shape, dtype in outs],
        in_specs=ins,
        out_specs=vm(len(outs)),
        scratch_shapes=list(scratch),
        cost_estimate=pl.CostEstimate(flops=1000000, bytes_accessed=0, transcendentals=0),
        name=name,
        compiler_params=pltpu.CompilerParams(vmem_limit_bytes=int(mib * MIB)),
    )


def per_device(
    queries, token_latents, key_rotary, latent_norm_gain, latent_up_weight, w_out,
    tokens_b, moe_gain, group_logits, inner_logits, expert_pick, w_gate, w_up, w_down,
):
    ep = ("z", "x")
    zs, xs, ys = lax.axis_size("z"), lax.axis_size("x"), lax.axis_size("y")
    z, x, c = (lax.axis_index(n).astype(jnp.int32) for n in ("z", "x", "c"))
    tok = queries.shape[0]
    width = tokens_b.shape[1]
    experts = zs * xs
    half = 8
    slots = experts * half
    ff = w_gate.shape[2]
    swap = [(0, 1), (1, 0)]

    positions = ((z * xs + x) * tok + jnp.arange(tok, dtype=jnp.int32)).astype(F32)
    freq = jnp.power(10000.0, -jnp.arange(ROT // 2, dtype=F32) * 2.0 / ROT)
    ang = freq[:, None] * positions[None, :]
    cos, sin = jnp.cos(ang), jnp.sin(ang)

    where = jnp.stack([z, x, c])
    cs = c.reshape(1)
    (outbound,) = call(
        rows_kernel, "rows", [((slots, width), BF)], SM + hb(3), 63.9,
        [
            pltpu.VMEM((tok, width), BF), pltpu.VMEM((1, width), F32), pltpu.VMEM((2, tok), jnp.int32),
            pltpu.SemaphoreType.DMA((3,)),
        ],
    )(cs, tokens_b, moe_gain[None, :], expert_pick.T)
    arrived = lax.all_to_all(outbound.reshape(experts, half, width), ep, 0, 0, tiled=True)

    wg, wu, wd = w_gate[0], w_up[0], w_down[0]
    wg2, wu2, wd2 = (lax.ppermute(w, "c", swap) for w in (wg, wu, wd))

    lat_w = token_latents.shape[1]
    pack, spread = call(
        keys_kernel, "keys", [((zs, PLAIN + ROT + VAL, tok), BF), ((tok, 4 * slots), BF)],
        hb(2) + vm(2) + hb(5), 16,
        [
            pltpu.VMEM((tok, lat_w), BF), pltpu.VMEM((ROT, tok), BF), pltpu.VMEM((1, lat_w), F32),
            pltpu.VMEM((lat_w, PLAIN + VAL), BF), pltpu.VMEM((2, tok), jnp.int32),
            pltpu.VMEM((GROUPS, tok), F32), pltpu.VMEM((2, tok), F32), pltpu.SemaphoreType.DMA((7,)),
        ],
    )(
        token_latents, key_rotary.T, cos, sin, latent_norm_gain[None, :], latent_up_weight,
        expert_pick.T, group_logits.T, inner_logits.T,
    )
    (q_own,) = call(query_kernel, "query", [((tok, PLAIN + ROT), BF)], vm(3), 16)(queries.T, cos, sin)
    qs = [q_own] + [
        lax.ppermute(q_own, "x", [(i, (i + k) % xs) for i in range(xs)]) for k in range(1, xs)
    ]
    arrived, pack, qs = lax.optimization_barrier((arrived, pack, qs))
    kv_all = lax.all_to_all(pack, "z", 0, 0, tiled=True)
    into = pltpu.VMEM((width, 2 * ff), BF)
    hid, down, down2 = call(
        hidden_kernel, "hidden", [((slots, 2 * ff), BF), ((ff, width // 2), BF), ((ff, width // 2), BF)],
        SM + vm(1) + hb(6), 32, [into, into, pltpu.SemaphoreType.DMA((4 + 2 * ys,))],
    )(cs, arrived.reshape(slots, width), wg, wu, wg2, wu2, wd, wd2)
    hid2 = lax.ppermute(hid, "c", swap)
    (result,) = call(down_kernel, "down", [((slots, width), BF)], SM + vm(4), 24)(
        cs, hid, hid2, down, down2
    )
    result, kv_all = lax.optimization_barrier((result, kv_all))
    returned = lax.all_to_all(result.reshape(experts, half, width), ep, 0, 0, tiled=True)
    parts = call(attend_kernel, "attend", [((tok, 128), BF)] * xs, SM + vm(5), 16)(where, *qs, kv_all)
    back = [parts[0]] + [
        lax.ppermute(parts[k], "x", [(i, (i - k) % xs) for i in range(xs)]) for k in range(1, xs)
    ]
    keep_mix, send_mix = call(
        mix_kernel, "mix", [((ys, 8, width), BF)] * 2, SM + vm(5), 16, [pltpu.VMEM((tok, width), F32)]
    )(where, *back, w_out)
    got_mix = lax.ppermute(send_mix, "c", swap)
    mix_half = (keep_mix.astype(F32) + got_mix.astype(F32)).astype(BF)
    mix_rows = mix_half.reshape(ys, 8, width // 128, 128).transpose(0, 2, 1, 3).reshape(ys, width // 16, 128)

    returned, mix_rows = lax.optimization_barrier((returned, mix_rows))
    (partial_sums,) = call(combine_kernel, "combine", [((ys, 2 * tok, 128), BF)], vm(3), 16)(
        returned.reshape(slots, width), spread, mix_rows
    )
    last = lax.all_to_all(partial_sums, "y", 0, 0, tiled=True)
    summed = jnp.sum(last.astype(F32), axis=0).astype(BF)
    expert_out = summed[:tok]
    mixer_out = summed[tok:].reshape(width // 128, 8, 128).transpose(1, 0, 2).reshape(8, width)
    return mixer_out, expert_out


def solution(mesh):
    fine = Mesh(mesh.devices.reshape(8, 4, 8, 2), ("z", "x", "y", "c"))
    e, t = ("z", "x"), ("y", "c")
    in_specs = (
        P(e, t), P(e, None), P(e, None), P(), P(None, t), P(t, None), P(e, None), P(),
        P(e, None), P(e, None), P(e, None), P(e, None, t), P(e, None, t), P(e, t, None),
    )
    out_specs = (P(e + t, None), P(e, t))
    return jax.shard_map(per_device, mesh=fine, in_specs=in_specs, out_specs=out_specs, check_vma=False)
```

```python
import functools

import jax
import jax.numpy as jnp
from jax import lax
from jax.experimental import pallas as pl
from jax.experimental.pallas import tpu as pltpu
from jax.sharding import Mesh, PartitionSpec as P

PLAIN = 64
ROT = 32
VAL = 64
SEG = 64
GROUPS = 4
BF = jnp.bfloat16
F32 = jnp.float32
MIB = 1024 * 1024


def turn(v, cos, sin):
    a, b = v[: ROT // 2].astype(F32), v[ROT // 2 :].astype(F32)
    return jnp.concatenate([a * cos - b * sin, b * cos + a * sin], axis=0)


def fetch(pairs, sems):
    copies = [pltpu.make_async_copy(src, dst, sems.at[i]) for i, (src, dst) in enumerate(pairs)]
    for cp in copies:
        cp.start()
    return copies


def choose(pick_ref, experts, base, count):
    tok = pick_ref.shape[1]
    eid = lax.broadcasted_iota(jnp.int32, (experts, tok), 0)
    hit0, hit1 = eid == pick_ref[0:1, :], eid == pick_ref[1:2, :]
    hit = hit0 | hit1
    before = lax.broadcasted_iota(jnp.int32, (tok, tok), 0) < lax.broadcasted_iota(jnp.int32, (tok, tok), 1)
    rank = jnp.dot(
        jnp.where(hit, 1.0, 0.0).astype(BF), jnp.where(before, 1.0, 0.0).astype(BF), preferred_element_type=F32
    )
    code = jnp.where(hit, rank, -1.0)
    slot = (lax.broadcasted_iota(jnp.int32, (count, tok), 0) + base).astype(F32)
    sel = jnp.concatenate([jnp.where(code[e : e + 1, :] == slot, 1.0, 0.0) for e in range(experts)], axis=0)
    return hit0, hit1, sel


def keys_kernel(
    lat_hbm, rot_hbm, cos_ref, sin_ref, gain_hbm, up_hbm, pick_hbm, gl_hbm, il_hbm,
    o_ref, w_ref, lat_ref, rot_ref, gain_ref, up_ref, pick_ref, gl_ref, il_ref, sems,
):
    pairs = (
        (lat_hbm, lat_ref), (gain_hbm, gain_ref), (up_hbm, up_ref), (rot_hbm, rot_ref),
        (pick_hbm, pick_ref), (gl_hbm, gl_ref), (il_hbm, il_ref),
    )
    for cp in fetch(pairs, sems):
        cp.wait()
    lat = lat_ref[...].astype(F32)
    lat = (lat * lax.rsqrt(jnp.mean(lat * lat, axis=1, keepdims=True) + 1e-06) * gain_ref[...]).astype(BF)
    kv = jnp.dot(lat, up_ref[...], preferred_element_type=F32).T
    rot = turn(rot_ref[...], cos_ref[...], sin_ref[...])
    pack = jnp.concatenate([kv[:PLAIN], rot, kv[PLAIN:]], axis=0).astype(BF)
    for b in range(o_ref.shape[0]):
        o_ref[b] = pack

    experts = w_ref.shape[1] // 32
    tok = w_ref.shape[0]
    hit0, hit1, low = choose(pick_ref, experts, 0, 8)
    _, _, high = choose(pick_ref, experts, 8, 8)
    gl = gl_ref[...]
    home = pick_ref[0:1, :] // (experts // GROUPS)
    gid = lax.broadcasted_iota(jnp.int32, (GROUPS, tok), 0)
    own = jnp.sum(jnp.where(gid == home, gl, 0.0), axis=0, keepdims=True)
    share = 1.0 / jnp.sum(jnp.exp(gl - own), axis=0, keepdims=True)
    gap = il_ref[0:1, :] - il_ref[1:2, :]
    first = share * (1.0 / (1.0 + jnp.exp(-gap)))
    second = share * (1.0 / (1.0 + jnp.exp(gap)))
    weight = jnp.where(hit0, first, 0.0) + jnp.where(hit1, second, 0.0)
    each = jnp.concatenate([jnp.broadcast_to(weight[e : e + 1, :], (8, tok)) for e in range(experts)], axis=0)
    spread = jnp.concatenate([low * each, high * each], axis=0)
    hi = spread.astype(BF).astype(F32)
    w_ref[...] = jnp.concatenate([hi, spread - hi], axis=0).T.astype(BF)


def rows_kernel(c_ref, tok_hbm, gain_hbm, pick_hbm, o_ref, tok_ref, gain_ref, pick_ref, sems):
    cps = fetch(((pick_hbm, pick_ref), (tok_hbm, tok_ref), (gain_hbm, gain_ref)), sems)
    cps[0].wait()
    _, _, sel = choose(pick_ref, o_ref.shape[0] // 8, 8 * c_ref[0], 8)
    cps[1].wait()
    cps[2].wait()
    vals = tok_ref[...].astype(F32)
    cen = vals - jnp.mean(vals, axis=1, keepdims=True)
    var = jnp.mean(cen * cen, axis=1, keepdims=True)
    normed = (cen * lax.rsqrt(var + 1e-05) * gain_ref[...]).astype(BF)
    o_ref[...] = jnp.dot(sel.astype(BF), normed, preferred_element_type=F32).astype(BF)


def split3(v):
    hi = v.astype(BF).astype(F32)
    rest = v - hi
    mid = rest.astype(BF).astype(F32)
    return hi, mid, rest - mid


def query_kernel(q_ref, cos_ref, sin_ref, o_ref):
    q = jnp.concatenate([q_ref[:PLAIN].astype(F32), turn(q_ref[PLAIN:], cos_ref[...], sin_ref[...])], axis=0)
    o_ref[...] = q.T.astype(BF)


def attend_kernel(where_ref, q0, q1, q2, q3, kv_ref, o0, o1, o2, o3):
    z, x = where_ref[0], where_ref[1]
    xs = 4
    zs, _, tok = kv_ref.shape
    segs = tok // SEG
    keys = jnp.concatenate([kv_ref[b, : PLAIN + ROT, :] for b in range(zs)], axis=1)
    vals = jnp.concatenate([kv_ref[b, PLAIN + ROT :, :] for b in range(zs)], axis=1)
    col = lax.broadcasted_iota(jnp.int32, (1, zs * tok), 1)
    key_seg = ((col // tok) * xs + x) * segs + (col % tok) // SEG
    row = lax.broadcasted_iota(jnp.int32, (tok, 1), 0)
    scale = (PLAIN + ROT) ** -0.5
    lane = lax.broadcasted_iota(jnp.int32, (tok, 128), 1)
    for k, (q_ref, o_ref) in enumerate(((q0, o0), (q1, o1), (q2, o2), (q3, o3))):
        xq = lax.rem(x + xs - k, xs)
        q_seg = (z * xs + xq) * segs + row // SEG
        s = jnp.dot(q_ref[...], keys, preferred_element_type=F32) * scale
        s = jnp.where(q_seg >= key_seg, s, -3e38)
        m = jnp.maximum(jnp.max(s, axis=1, keepdims=True), -1e30)
        p = jnp.exp(s - m)
        l = jnp.sum(p, axis=1, keepdims=True)
        acc = lax.dot_general(p.astype(BF), vals, (((1,), (1,)), ((), ())), preferred_element_type=F32)
        out = jnp.concatenate([acc, jnp.zeros((tok, 128 - VAL), F32)], axis=1)
        for i, piece in enumerate(split3(m) + split3(l)):
            out = jnp.where(lane == VAL + i, piece, out)
        o_ref[...] = out.astype(BF)


def mix_kernel(where_ref, a0, a1, a2, a3, w_ref, keep_ref, send_ref, res_ref):
    c = where_ref[2]
    parts = [r[...].astype(F32) for r in (a0, a1, a2, a3)]
    ms = [p[:, VAL : VAL + 1] + p[:, VAL + 1 : VAL + 2] + p[:, VAL + 2 : VAL + 3] for p in parts]
    ls = [p[:, VAL + 3 : VAL + 4] + p[:, VAL + 4 : VAL + 5] + p[:, VAL + 5 : VAL + 6] for p in parts]
    m = functools.reduce(jnp.maximum, ms)
    total = denom = 0.0
    for p, mp, lp in zip(parts, ms, ls):
        w = jnp.exp(mp - m)
        total = total + w * p[:, :VAL]
        denom = denom + w * lp
    attended = (total / denom).astype(BF)
    res_ref[...] = jnp.dot(attended, w_ref[...], preferred_element_type=F32)
    for y in range(keep_ref.shape[0]):
        keep_ref[y] = res_ref[pl.ds(pl.multiple_of(16 * y + 8 * c, 8), 8), :].astype(BF)
        send_ref[y] = res_ref[pl.ds(pl.multiple_of(16 * y + 8 * (1 - c), 8), 8), :].astype(BF)


def hidden_kernel(c_ref, x_ref, g0h, u0h, g1h, u1h, d2h, o_ref, d2, gu0, gu1, sems):
    c = c_ref[0]
    f = o_ref.shape[1] // 2
    pairs = [(g0h, gu0.at[:, :f]), (u0h, gu0.at[:, f:]), (g1h, gu1.at[:, :f]), (u1h, gu1.at[:, f:])]
    for y in range(d2.shape[1] // 128):
        cols = pl.ds(pl.multiple_of(128 * (2 * y + c), 128), 128)
        pairs.append((d2h.at[:, cols], d2.at[:, 128 * y : 128 * y + 128]))
    cps = fetch(pairs, sems)
    rows = x_ref[...]
    for i, gu_ref in enumerate((gu0, gu1)):
        cps[2 * i].wait()
        cps[2 * i + 1].wait()
        both = jnp.dot(rows, gu_ref[...], preferred_element_type=F32)
        g, u = both[:, :f], both[:, f:]
        o_ref[:, i * f : (i + 1) * f] = (g / (1.0 + jnp.exp(-g)) * u).astype(BF)
    for cp in cps[4:]:
        cp.wait()


def down_kernel(c_ref, h_ref, h2_ref, dh, d2, o_ref, d, sems):
    c = c_ref[0]
    f = d.shape[0]
    pairs = []
    for y in range(d.shape[1] // 128):
        cols = pl.ds(pl.multiple_of(128 * (2 * y + c), 128), 128)
        pairs.append((dh.at[:, cols], d.at[:, 128 * y : 128 * y + 128]))
    for cp in fetch(pairs, sems):
        cp.wait()
    for i, h, first, second in ((c, h_ref, d, d2), (1 - c, h2_ref, d2, d)):
        acc = jnp.dot(h[:, :f], first[...], preferred_element_type=F32) + jnp.dot(
            h[:, f:], second[...], preferred_element_type=F32
        )
        wide = d.shape[1]
        o_ref[:, pl.ds(pl.multiple_of(wide * i, 128), wide)] = acc.astype(BF)


def combine_kernel(r_ref, w_ref, mix_ref, o_ref):
    tok = w_ref.shape[0]
    wide = r_ref.shape[1] // 2
    both = jnp.concatenate([r_ref[:, :wide], r_ref[:, wide:]] * 2, axis=0)
    out = jnp.dot(w_ref[...], both, preferred_element_type=F32)
    for y in range(o_ref.shape[0]):
        o_ref[y, :tok] = out[:, 128 * y : 128 * (y + 1)].astype(BF)
        o_ref[y, tok:] = mix_ref[y]


def vm(n):
    return [pl.BlockSpec(memory_space=pltpu.VMEM)] * n


def hb(n):
    return [pl.BlockSpec(memory_space=pltpu.HBM)] * n


SM = [pl.BlockSpec(memory_space=pltpu.SMEM)]


def call(kernel, name, outs, ins, mib, scratch=()):
    return pl.pallas_call(
        kernel,
        out_shape=[jax.ShapeDtypeStruct(shape, dtype) for shape, dtype in outs],
        in_specs=ins,
        out_specs=vm(len(outs)),
        scratch_shapes=list(scratch),
        cost_estimate=pl.CostEstimate(flops=1000000, bytes_accessed=0, transcendentals=0),
        name=name,
        compiler_params=pltpu.CompilerParams(vmem_limit_bytes=int(mib * MIB)),
    )


def per_device(
    queries, token_latents, key_rotary, latent_norm_gain, latent_up_weight, w_out,
    tokens_b, moe_gain, group_logits, inner_logits, expert_pick, w_gate, w_up, w_down,
):
    ep = ("z", "x")
    zs, xs, ys = lax.axis_size("z"), lax.axis_size("x"), lax.axis_size("y")
    z, x, c = (lax.axis_index(n).astype(jnp.int32) for n in ("z", "x", "c"))
    tok = queries.shape[0]
    width = tokens_b.shape[1]
    experts = zs * xs
    half = 8
    slots = experts * half
    ff = w_gate.shape[2]
    swap = [(0, 1), (1, 0)]

    positions = ((z * xs + x) * tok + jnp.arange(tok, dtype=jnp.int32)).astype(F32)
    freq = jnp.power(10000.0, -jnp.arange(ROT // 2, dtype=F32) * 2.0 / ROT)
    ang = freq[:, None] * positions[None, :]
    cos, sin = jnp.cos(ang), jnp.sin(ang)

    where = jnp.stack([z, x, c])
    cs = c.reshape(1)
    (outbound,) = call(
        rows_kernel, "rows", [((slots, width), BF)], SM + hb(3), 63.9,
        [
            pltpu.VMEM((tok, width), BF), pltpu.VMEM((1, width), F32), pltpu.VMEM((2, tok), jnp.int32),
            pltpu.SemaphoreType.DMA((3,)),
        ],
    )(cs, tokens_b, moe_gain[None, :], expert_pick.T)
    arrived = lax.all_to_all(outbound.reshape(experts, half, width), ep, 0, 0, tiled=True)

    wg, wu, wd = w_gate[0], w_up[0], w_down[0]
    wg2, wu2, wd2 = (lax.ppermute(w, "c", swap) for w in (wg, wu, wd))

    lat_w = token_latents.shape[1]
    pack, spread = call(
        keys_kernel, "keys", [((zs, PLAIN + ROT + VAL, tok), BF), ((tok, 4 * slots), BF)],
        hb(2) + vm(2) + hb(5), 16,
        [
            pltpu.VMEM((tok, lat_w), BF), pltpu.VMEM((ROT, tok), BF), pltpu.VMEM((1, lat_w), F32),
            pltpu.VMEM((lat_w, PLAIN + VAL), BF), pltpu.VMEM((2, tok), jnp.int32),
            pltpu.VMEM((GROUPS, tok), F32), pltpu.VMEM((2, tok), F32), pltpu.SemaphoreType.DMA((7,)),
        ],
    )(
        token_latents, key_rotary.T, cos, sin, latent_norm_gain[None, :], latent_up_weight,
        expert_pick.T, group_logits.T, inner_logits.T,
    )
    (q_own,) = call(query_kernel, "query", [((tok, PLAIN + ROT), BF)], vm(3), 16)(queries.T, cos, sin)
    qs = [q_own] + [
        lax.ppermute(q_own, "x", [(i, (i + k) % xs) for i in range(xs)]) for k in range(1, xs)
    ]
    arrived, pack, qs = lax.optimization_barrier((arrived, pack, qs))
    kv_all = lax.all_to_all(pack, "z", 0, 0, tiled=True)
    into = pltpu.VMEM((width, 2 * ff), BF)
    hid, down2 = call(
        hidden_kernel, "hidden", [((slots, 2 * ff), BF), ((ff, width // 2), BF)],
        SM + vm(1) + hb(5), 32, [into, into, pltpu.SemaphoreType.DMA((4 + ys,))],
    )(cs, arrived.reshape(slots, width), wg, wu, wg2, wu2, wd2)
    hid2 = lax.ppermute(hid, "c", swap)
    (result,) = call(
        down_kernel, "down", [((slots, width), BF)], SM + vm(2) + hb(1) + vm(1), 24,
        [pltpu.VMEM((ff, width // 2), BF), pltpu.SemaphoreType.DMA((ys,))],
    )(cs, hid, hid2, wd, down2)
    result, kv_all = lax.optimization_barrier((result, kv_all))
    returned = lax.all_to_all(result.reshape(experts, half, width), ep, 0, 0, tiled=True)
    parts = call(attend_kernel, "attend", [((tok, 128), BF)] * xs, SM + vm(5), 16)(where, *qs, kv_all)
    back = [parts[0]] + [
        lax.ppermute(parts[k], "x", [(i, (i - k) % xs) for i in range(xs)]) for k in range(1, xs)
    ]
    keep_mix, send_mix = call(
        mix_kernel, "mix", [((ys, 8, width), BF)] * 2, SM + vm(5), 16, [pltpu.VMEM((tok, width), F32)]
    )(where, *back, w_out)
    got_mix = lax.ppermute(send_mix, "c", swap)
    mix_half = (keep_mix.astype(F32) + got_mix.astype(F32)).astype(BF)
    mix_rows = mix_half.reshape(ys, 8, width // 128, 128).transpose(0, 2, 1, 3).reshape(ys, width // 16, 128)

    returned, mix_rows = lax.optimization_barrier((returned, mix_rows))
    (partial_sums,) = call(combine_kernel, "combine", [((ys, 2 * tok, 128), BF)], vm(3), 16)(
        returned.reshape(slots, width), spread, mix_rows
    )
    last = lax.all_to_all(partial_sums, "y", 0, 0, tiled=True)
    summed = jnp.sum(last.astype(F32), axis=0).astype(BF)
    expert_out = summed[:tok]
    mixer_out = summed[tok:].reshape(width // 128, 8, 128).transpose(1, 0, 2).reshape(8, width)
    return mixer_out, expert_out


def solution(mesh):
    fine = Mesh(mesh.devices.reshape(8, 4, 8, 2), ("z", "x", "y", "c"))
    e, t = ("z", "x"), ("y", "c")
    in_specs = (
        P(e, t), P(e, None), P(e, None), P(), P(None, t), P(t, None), P(e, None), P(),
        P(e, None), P(e, None), P(e, None), P(e, None, t), P(e, None, t), P(e, t, None),
    )
    out_specs = (P(e + t, None), P(e, t))
    return jax.shard_map(per_device, mesh=fine, in_specs=in_specs, out_specs=out_specs, check_vma=False)
```
